256 devices in a mesh: sp: 16 (over y, x), tp: 16 (over z, core).
Axes of the slice: x: 4, y: 4, z: 8, core: 2. Of those that a mesh axis runs over, the one named last changes fastest.
Arguments:
- queries: bfloat16 [12288, 16, 128], P('sp', 'tp'), may hold values from -240 to 240
- key_pairs: bfloat16 [12288, 16, 128], P('sp', 'tp'), may hold values from -11 to 11
- head_values: bfloat16 [12288, 16, 128], P('sp', 'tp'), may hold values from -6 to 6
- lambdas: float32 [16], P('tp'), may hold values from 0.3 to 0.8
- head_gain: float32 [128], replicated, may hold values from 0.1 to 1.9
- out_weight: bfloat16 [2048, 2048], replicated, may hold values from -0.125 to 0.125
- residual: bfloat16 [12288, 2048], P(('sp', 'tp')), may hold values from -6 to 6
- norm_gain: float32 [2048], replicated, may hold values from 0.1 to 1.9
- expert_ids: int32 [12288, 2], P(('sp', 'tp')), may hold values from 0 to 31, all different within a row; in each aligned block of 48 rows (0 to 47, 48 to 95, ...) at most 4 rows name the same one
- route_weights: float32 [12288, 2], P(('sp', 'tp')), may hold values from 0.2 to 1
- gate_weight: bfloat16 [32, 2048, 2048], P('sp', None, 'tp'), may hold values from -0.125 to 0.125
- up_weight: bfloat16 [32, 2048, 2048], P('sp', None, 'tp'), may hold values from -0.125 to 0.125
- down_weight: bfloat16 [32, 2048, 2048], P('sp', 'tp'), may hold values from -0.125 to 0.125
Outputs:
- merged: bfloat16 [12288, 2048], P(('sp', 'tp'))
The draws below stay inside these ranges and needn't reach their ends.
Inputs may be any that keep to these rules, and one draw needn't show every extreme that they name: `expert_ids`: within the rows of one device each expert is named at most 4 times, and exactly 4 times in some device.
All inputs are finite; a program needn't handle non-finite values.
Results may differ from the reference program's by a relative error of at most 0.019.
Values may be sent and summed in bfloat16 or wider, within the bound.
A program may use at most 128 MiB of HBM per device.

```python
import math
import jax
import jax.numpy as jnp
import numpy as np
from jax import lax

D = 2048
HEADS = 16
HD = 64
VD = 128
FF = 2048
TOPK = 2
LENGTH = 12288
ROWS = 48
EXPERTS = 32
CAP = 4
N_TP = 16


def base_field(key, salt_value):
    return jnp.clip(jax.random.normal(jax.random.fold_in(key, salt_value), (LENGTH, HEADS, 2 * HD), jnp.float32), -4.0, 4.0) * 1.3


def draw_key_pairs(key, part):
    drawn_field = base_field(key, 11)
    return drawn_field.astype(jnp.bfloat16)


def draw_queries(key, part):
    drawn_field = base_field(key, 12)
    return drawn_field.astype(jnp.bfloat16)


def block_levels(rng, dims, shards, smallest, largest):
    loudness = 1.0
    for dim, blocks in shards:
        draws = jax.random.uniform(jax.random.fold_in(jax.random.fold_in(rng, 6), dim), (blocks,), jnp.float32, smallest / len(shards), largest / len(shards))
        loudness = loudness * jnp.repeat(jnp.exp(draws), dims[dim] // blocks).reshape((-1,) + (1,) * (len(dims) - 1 - dim))
    return loudness


def shared_out(own_key, own, number, rows, amount, top, limit, lean):
    order = jax.random.permutation(own_key, amount)
    crowded, common = load_shares(amount, rows * top, limit, lean, True), load_shares(amount, rows * top, limit, lean, False)
    places = jnp.arange(amount)

    def named(sizes, rotation):
        used = int((sizes > 0).sum())
        fixed = max(1, used // 4)
        passed = fixed + (places - fixed + rotation * (used - fixed)) % max(1, amount - fixed)
        return jnp.zeros((amount,), jnp.int32).at[order[jnp.where(places < fixed, places, passed)]].set(jnp.asarray(sizes, jnp.int32))

    sizes = jnp.where(number % 4 == 0, named(crowded, number // 4), named(common, number - number // 4 - 1))
    mixed = jax.random.permutation(jax.random.fold_in(own, 3), amount)
    source_of, sink = mixed[0:amount // 2 * 2:2], mixed[1:amount // 2 * 2:2]
    room = jnp.minimum(sizes[source_of] - 1, limit - sizes[sink]) // 2
    room = jnp.where((source_of == order[0]) | (sink == order[0]) | (sizes[sink] == 0), 0, jnp.maximum(room, 0))
    passed = jax.random.randint(jax.random.fold_in(own, 4), (amount // 2,), 0, 1 << 20) % (room + 1)
    sizes = sizes.at[source_of].add(-passed).at[sink].add(passed)
    items = jnp.searchsorted(jnp.cumsum(sizes), jnp.arange(rows * top), side="right").astype(jnp.int32)
    table = items.reshape(top, rows).T
    table = table[jax.random.permutation(jax.random.fold_in(own, 1), rows)]
    rotation = jax.random.randint(jax.random.fold_in(own, 2), (rows, 1), 0, top)
    return jnp.take_along_axis(table, (jnp.arange(top)[None, :] + rotation) % top, axis=1)


def load_shares(count, total, limit, skew, full):
    portions = [(1 << 20) // math.isqrt(grade ** skew) + 1 for grade in range(1, count + 1)]
    largest = limit if full else min(limit, max(-(-total // count), total * portions[0] // sum(portions)))
    least = 1 if total - largest >= count - 1 else 0
    holding, surplus = [largest] + [least] * (count - 1), total - largest - least * (count - 1)
    while surplus > 0:
        free = [i for i in range(1, count) if holding[i] < largest] or [i for i in range(1, count) if holding[i] < limit]
        mass, budget = sum([portions[i] for i in free]), surplus
        for i in free:
            more = min(limit - holding[i], max(1, budget * portions[i] // mass), surplus)
            holding[i] = holding[i] + more
            surplus = surplus - more
    return np.array(holding)


def centred(own_key, extent, scale, most, cuts=(), kind=jnp.bfloat16):
    loudness = block_levels(own_key, extent, cuts, -0.22, 0.18) if cuts else 1.0
    values = jax.random.normal(own_key, extent, jnp.float32) * scale * loudness
    return jnp.minimum(jnp.maximum(values, -most), most).astype(kind)


def setup_inputs(seed: int = 0) -> dict:
    key_list = jax.random.split(jax.random.key(seed), 14)
    queries = draw_queries(jax.random.fold_in(key_list[13], 71), 0)
    key_pairs = draw_key_pairs(jax.random.fold_in(key_list[13], 71), 0)
    head_values = centred(key_list[2], (LENGTH, HEADS, VD), 1.0, 6.0, ((0, 16), (1, 16)))
    lambdas = jnp.clip(0.3 + 0.5 * jax.random.uniform(key_list[3], (HEADS,), jnp.float32) ** block_levels(key_list[3], (HEADS,), ((0, 16),), -0.2, 0.2), 0.3, 0.8)
    head_gain = jnp.clip(1.0 + 0.18 * jax.random.normal(key_list[4], (VD,), jnp.float32), 0.1, 1.9)
    out_weight = centred(key_list[5], (HEADS * VD, D), (HEADS * VD) ** -0.5, 0.125)
    residual = centred(key_list[6], (LENGTH, D), 1.0, 6.0, ((0, 256),))
    norm_gain = jnp.clip(1.0 + 0.18 * jax.random.normal(key_list[7], (D,), jnp.float32), 0.1, 1.9)
    expert_ids_keys = jax.random.split(jax.random.fold_in(key_list[8], 1), LENGTH // ROWS)
    expert_ids_turns = jax.random.permutation(jax.random.fold_in(key_list[8], 3), LENGTH // ROWS)
    expert_ids = jax.vmap(lambda own, number: shared_out(jax.random.fold_in(key_list[8], 2), own, number, ROWS, EXPERTS, TOPK, CAP, 1))(expert_ids_keys, expert_ids_turns).reshape((LENGTH, TOPK))
    route_weights = jnp.clip(0.2 + 0.8 * jax.random.uniform(key_list[9], (LENGTH, TOPK), jnp.float32) ** block_levels(key_list[9], (LENGTH, TOPK), ((0, 256),), -0.2, 0.2), 0.2, 1.0)
    gate_weight = centred(key_list[10], (EXPERTS, D, FF), D ** -0.5, 0.125, ((0, 16), (2, 16)))
    up_weight = centred(key_list[11], (EXPERTS, D, FF), D ** -0.5, 0.125, ((0, 16), (2, 16)))
    down_weight = centred(key_list[12], (EXPERTS, FF, D), FF ** -0.5, 0.125, ((0, 16), (1, 16)))
    return {"queries": queries, "key_pairs": key_pairs, "head_values": head_values, "lambdas": lambdas, "head_gain": head_gain, "out_weight": out_weight, "residual": residual, "norm_gain": norm_gain, "expert_ids": expert_ids, "route_weights": route_weights, "gate_weight": gate_weight, "up_weight": up_weight, "down_weight": down_weight}


def attend_head(query_rows, key_rows, value_rows, weight_two):
    block_rows = min(512, LENGTH)
    columns = jnp.arange(LENGTH, dtype=jnp.int32)

    def one_block(block_index):
        offset = block_index * block_rows
        query_block = lax.dynamic_slice_in_dim(query_rows, offset, block_rows, 0)
        positions = offset + jnp.arange(block_rows, dtype=jnp.int32)
        allowed = columns[None, :] <= positions[:, None]
        results = []
        for member in range(2):
            first_col = member * HD
            scores = jnp.dot(query_block[:, first_col:first_col + HD], key_rows[:, first_col:first_col + HD].T, preferred_element_type=jnp.float32) * HD ** (-0.5)
            scores = jnp.where(allowed, scores, -jnp.inf)
            highest = lax.optimization_barrier(jnp.max(scores, axis=1, keepdims=True))
            weights = jnp.exp(scores - highest)
            totals = lax.optimization_barrier(jnp.sum(weights, axis=1, keepdims=True))
            summed = jnp.dot(weights.astype(jnp.bfloat16), value_rows, preferred_element_type=jnp.float32)
            results.append(summed / totals)
        return results[0] - weight_two * results[1]
    blocks = lax.map(one_block, jnp.arange(LENGTH // block_rows, dtype=jnp.int32))
    return blocks.reshape(LENGTH, VD)

def reference(queries, key_pairs, head_values, lambdas, head_gain, out_weight, residual, norm_gain, expert_ids, route_weights, gate_weight, up_weight, down_weight):

    def one_head(packed):
        query_rows, key_rows, value_rows, weight_two = packed
        mixed = attend_head(query_rows, key_rows, value_rows, weight_two)
        row_scale = lax.rsqrt(lax.optimization_barrier(jnp.mean(mixed * mixed, axis=1, keepdims=True)) + 1e-06)
        return (mixed * row_scale * head_gain).astype(jnp.bfloat16)
    per_head = lax.map(one_head, (jnp.transpose(queries, (1, 0, 2)), jnp.transpose(key_pairs, (1, 0, 2)), jnp.transpose(head_values, (1, 0, 2)), lambdas))
    attended = jnp.transpose(per_head, (1, 0, 2)).reshape(LENGTH, HEADS * VD)
    projected = jnp.dot(attended, out_weight, preferred_element_type=jnp.float32)
    updated = (residual.astype(jnp.float32) + projected).astype(jnp.bfloat16)
    widened = updated.astype(jnp.float32)
    normed = (widened * lax.rsqrt(lax.optimization_barrier(jnp.mean(widened * widened, axis=1, keepdims=True)) + 1e-06) * norm_gain).astype(jnp.bfloat16)
    flat_ids = expert_ids.reshape(-1)
    flat_weights = route_weights.reshape(-1)
    owners = jnp.arange(LENGTH * TOPK, dtype=jnp.int32) // TOPK
    most_rows = LENGTH // ROWS * CAP
    slice_width = FF // N_TP

    def expert_step(gathered, expert):
        matches = flat_ids == expert
        chosen = jnp.nonzero(matches, size=most_rows, fill_value=0)[0].astype(jnp.int32)
        filled = (jnp.arange(most_rows, dtype=jnp.int32) < jnp.sum(matches.astype(jnp.int32))).astype(jnp.float32)
        targets = owners[chosen]
        inputs = normed[targets]
        gate_part = jnp.dot(inputs, gate_weight[expert], preferred_element_type=jnp.float32)
        up_part = jnp.dot(inputs, up_weight[expert], preferred_element_type=jnp.float32)
        inner_rows = (jax.nn.silu(gate_part) * up_part).astype(jnp.bfloat16)
        pieces = jnp.einsum('mtf,tfd->mtd', inner_rows.reshape(most_rows, N_TP, slice_width).astype(jnp.float32), down_weight[expert].reshape(N_TP, slice_width, D).astype(jnp.float32))
        pieces = lax.optimization_barrier(pieces.astype(jnp.bfloat16)).astype(jnp.float32)
        result = lax.optimization_barrier(lax.optimization_barrier(jnp.sum(pieces, axis=1)).astype(jnp.bfloat16)).astype(jnp.float32)
        scaled = result * (flat_weights[chosen] * filled)[:, None]
        return (gathered.at[targets].add(scaled), None)
    moe_sum, leftover = lax.scan(expert_step, jnp.zeros((LENGTH, D), jnp.float32), jnp.arange(EXPERTS, dtype=jnp.int32))
    return (updated.astype(jnp.float32) + moe_sum).astype(jnp.bfloat16)
```

```python
import functools

import jax
import jax.numpy as jnp
from jax import lax
from jax.experimental import pallas as pl
from jax.experimental.pallas import tpu as pltpu
from jax.sharding import PartitionSpec as P

MESH = pl.DeviceIdType.MESH
SIDE = 4
N_SP = 16
N_TP = 16
ROWS = 48
SPAN = N_TP * ROWS
HALF = SPAN // 2
GROUP = 2 * ROWS
TILE_GROUPS = 4
TILE = TILE_GROUPS * GROUP
LANES = 128
HD = 64
DEPTH = 2048
EXPERTS = 32
CAP = 4
SLOTS = EXPERTS * CAP
COLS = 512
NEG = -1e30

ORDER = [
    (0, 0), (-1, 0), (1, 0), (0, -1), (0, 1), (2, 0), (-1, -1), (-1, 1),
    (1, -1), (1, 1), (2, -1), (2, 1), (0, 2), (-1, 2), (1, 2), (2, 2),
]
PLACE = {0: 0, -1: 1, 1: 2, 2: 3}


def pick(index, values):
    out = jnp.int32(values[0])
    for k, value in enumerate(values):
        out = jnp.where(index == k, jnp.int32(value), out)
    return out


def mod(value, size):
    return lax.rem(value + size, size)


def attend_kernel(
    q_hbm, kv_hbm, w_hbm, lam_ref, gain_ref, select_ref, residual_ref, norm_gain_ref,
    updated_ref, slots_ref,
    q_own, q_land, qs, kvb, acc, top, own_heads, heads, w_vmem,
    local_sem, q_send, q_recv, kv_send, kv_recv, head_send, head_recv,
):
    sp = lax.axis_index("sp")
    tp = lax.axis_index("tp")
    x, y = lax.rem(sp, SIDE), sp // SIDE

    barrier = pltpu.get_barrier_semaphore()
    load_w = pltpu.make_async_copy(w_hbm, w_vmem, local_sem.at[0])
    load_w.start()
    load_kv = pltpu.make_async_copy(kv_hbm, kvb.at[sp], local_sem.at[1])
    load_kv.start()
    load_q = pltpu.make_async_copy(q_hbm, q_own, local_sem.at[2])
    load_q.start()

    def greet_plane(d, carry):
        pl.semaphore_signal(
            barrier, inc=1, device_id=(lax.rem(sp + d, N_SP), tp), device_id_type=MESH
        )
        return carry

    lax.fori_loop(1, N_SP, greet_plane, 0)

    def greet_sources(h, carry):
        @pl.when(jnp.logical_or(tp != sp, h != tp))
        def _():
            pl.semaphore_signal(barrier, inc=1, device_id=(tp, h), device_id_type=MESH)

        return carry

    lax.fori_loop(0, N_TP, greet_sources, 0)
    pl.semaphore_wait(
        barrier, N_SP - 1 + N_TP - jnp.where(sp == tp, jnp.int32(1), jnp.int32(0))
    )

    load_q.wait()

    def q_copy(d):
        other = lax.rem(sp + d, N_SP)
        return pltpu.make_async_remote_copy(
            src_ref=q_own.at[other], dst_ref=q_land.at[sp],
            send_sem=q_send.at[d], recv_sem=q_recv.at[d],
            device_id=(other, tp), device_id_type=MESH,
        )

    def send_q(d, carry):
        q_copy(d).start()
        return carry

    lax.fori_loop(1, N_SP, send_q, 0)
    load_kv.wait()

    def block_of(half, du, dv):
        dx, dy = (du, dv) if half == 0 else (dv, du)
        return mod(y + dy, SIDE) * SIDE + mod(x + dx, SIDE)

    def kv_copy(half, index, block, part, du, dv):
        ref = kvb.at[block, half] if part is None else kvb.at[block, half, part]
        return pltpu.make_async_remote_copy(
            src_ref=ref, dst_ref=ref,
            send_sem=kv_send.at[half, index], recv_sem=kv_recv.at[half, index],
            device_id=(block_of(half, du, dv), tp), device_id_type=MESH,
        )

    def send(half, index, rel, part, du, dv):
        kv_copy(half, index, block_of(half, *rel), part, du, dv).start()

    def arrived(half, index, rel, part):
        kv_copy(half, index, block_of(half, *rel), part, 1, 0).wait_recv()

    for half in range(2):
        send(half, 0, (0, 0), None, 1, 0)
        send(half, 1, (0, 0), None, -1, 0)
        send(half, 4, (0, 0), None, 0, 1)
        send(half, 8, (0, 0), None, 0, -1)

    for own in range(N_SP):
        @pl.when(sp == own)
        def _():
            q_land[own] = q_own[own]

    lane = lax.broadcasted_iota(jnp.int32, (ROWS, LANES), 1)

    def wait_q(d, carry):
        q_copy(d).wait_recv()
        return carry

    lax.fori_loop(1, N_SP, wait_q, 0)

    def pack_q(g, carry):
        rows = q_land[g].astype(jnp.float32) * (HD**-0.5)
        qs[g, 0:ROWS] = jnp.where(lane < HD, rows, 0.0).astype(jnp.bfloat16)
        qs[g, ROWS:GROUP] = jnp.where(lane >= HD, rows, 0.0).astype(jnp.bfloat16)
        return carry

    lax.fori_loop(0, N_SP, pack_q, 0)
    acc[...] = jnp.zeros_like(acc)
    top[...] = jnp.full_like(top, NEG)

    row = lax.broadcasted_iota(jnp.int32, (TILE_GROUPS, GROUP, HALF), 1)
    row = jnp.where(row >= ROWS, row - ROWS, row)
    offset = (
        lax.broadcasted_iota(jnp.int32, (TILE_GROUPS, GROUP, HALF), 0) * SPAN
        + row
        - lax.broadcasted_iota(jnp.int32, (TILE_GROUPS, GROUP, HALF), 2)
    ).reshape(TILE, HALF)

    def tile_step(t, block, half, masked):
        rows = pl.ds(pl.multiple_of(t * TILE, TILE), TILE)
        q_tile = qs[pl.ds(t * TILE_GROUPS, TILE_GROUPS)].reshape(TILE, LANES)
        keys = kvb[block, half, 0]
        values = kvb[block, half, 1]
        scores = lax.dot_general(
            q_tile, keys, (((1,), (1,)), ((), ())), preferred_element_type=jnp.float32
        )
        if masked:
            ahead = block * SPAN + half * HALF - t * (TILE_GROUPS * SPAN) - sp * ROWS
            scores = jnp.where(offset >= ahead, scores, -jnp.inf)
        old_top = top[rows]
        new_top = jnp.maximum(old_top, jnp.max(scores, axis=1, keepdims=True))
        decay = jnp.exp(old_top - new_top)
        weights = jnp.exp(scores - new_top[:, 0:1]).astype(jnp.bfloat16)
        wide = jnp.concatenate([values, jnp.ones_like(values)], axis=1)
        fresh = jnp.dot(weights, wide, preferred_element_type=jnp.float32)
        acc[rows] = acc[rows] * jnp.concatenate([decay, decay], axis=1) + fresh
        top[rows] = new_top

    def use_block(block, half):
        first = block // TILE_GROUPS
        tile_step(first, block, half, True)

        def later(t, carry):
            tile_step(t, block, half, False)
            return carry

        lax.fori_loop(first + 1, N_SP // TILE_GROUPS, later, 0)

    def step(s, carry):
        def on(k, half):
            du, dv = ORDER[k]
            if k == 1:
                arrived(half, 0, (-1, 0), None)
                send(half, 2, (-1, 0), 0, 1, 0)
                send(half, 5, (-1, 0), None, 0, 1)
                send(half, 9, (-1, 0), None, 0, -1)
            elif k == 2:
                arrived(half, 1, (1, 0), None)
                send(half, 3, (1, 0), 1, -1, 0)
                send(half, 6, (1, 0), None, 0, 1)
                send(half, 10, (1, 0), None, 0, -1)
            elif k == 5:
                arrived(half, 2, (2, 0), 0)
                arrived(half, 3, (2, 0), 1)
                send(half, 7, (2, 0), None, 0, 1)
                send(half, 11, (2, 0), None, 0, -1)
            elif dv == -1:
                place = PLACE[du]
                arrived(half, 4 + place, (du, dv), None)
                send(half, 12 + place, (du, dv), 0, 0, 1)
            elif dv == 1:
                place = PLACE[du]
                arrived(half, 8 + place, (du, dv), None)
                send(half, 16 + place, (du, dv), 1, 0, -1)
            elif dv == 2:
                place = PLACE[du]
                arrived(half, 12 + place, (du, dv), 0)
                arrived(half, 16 + place, (du, dv), 1)

        for k in range(1, len(ORDER)):
            @pl.when(s == k)
            def _():
                for half in range(2):
                    on(k, half)

        du = pick(s, [o[0] for o in ORDER])
        dv = pick(s, [o[1] for o in ORDER])

        def one_half(half, carry):
            dx = jnp.where(half == 0, du, dv)
            dy = jnp.where(half == 0, dv, du)
            block = mod(y + dy, SIDE) * SIDE + mod(x + dx, SIDE)
            use_block(block, half)
            return carry

        return lax.fori_loop(0, 2, one_half, carry)

    lax.fori_loop(0, len(ORDER), step, 0)

    lam = lam_ref[0, 0]

    def finish(g, carry):
        part = acc[pl.ds(pl.multiple_of(g * GROUP, GROUP), GROUP)]
        ratio = part[:, 0:LANES] / part[:, LANES : 2 * LANES]
        mixed = ratio[0:ROWS] - lam * ratio[ROWS:GROUP]
        square = jnp.mean(mixed * mixed, axis=1, keepdims=True)
        own_heads[g] = (mixed * lax.rsqrt(square + 1e-06) * gain_ref[...]).astype(
            jnp.bfloat16
        )
        return carry

    lax.fori_loop(0, N_SP, finish, 0)

    def head_copy(g, h):
        return pltpu.make_async_remote_copy(
            src_ref=own_heads.at[g],
            dst_ref=heads.at[:, pl.ds(pl.multiple_of(tp * LANES, LANES), LANES)],
            send_sem=head_send.at[g], recv_sem=head_recv.at[h],
            device_id=(g, sp), device_id_type=MESH,
        )

    def push_head(g, carry):
        @pl.when(jnp.logical_or(g != sp, sp != tp))
        def _():
            head_copy(g, tp).start()

        return carry

    lax.fori_loop(0, N_SP, push_head, 0)

    for own in range(N_SP):
        @pl.when(jnp.logical_and(sp == own, tp == own))
        def _():
            heads[:, own * LANES : (own + 1) * LANES] = own_heads[own]

    load_w.wait()

    def wait_head(h, carry):
        @pl.when(jnp.logical_or(h != tp, sp != tp))
        def _():
            head_copy(0, h).wait_recv()

        return carry

    lax.fori_loop(0, N_TP, wait_head, 0)

    attended = heads[...]
    squares = jnp.zeros((ROWS, 1), jnp.float32)
    wide = []
    for n in range(DEPTH // COLS):
        cols = slice(n * COLS, (n + 1) * COLS)
        projected = jnp.dot(attended, w_vmem[:, cols], preferred_element_type=jnp.float32)
        updated = (residual_ref[:, cols].astype(jnp.float32) + projected).astype(jnp.bfloat16)
        updated_ref[:, cols] = updated
        back = updated.astype(jnp.float32)
        squares = squares + jnp.sum(back * back, axis=1, keepdims=True)
        wide.append(back)
    scale = lax.rsqrt(squares / DEPTH + 1e-06)
    for n in range(DEPTH // COLS):
        cols = slice(n * COLS, (n + 1) * COLS)
        normed = (wide[n] * scale * norm_gain_ref[:, cols]).astype(jnp.bfloat16)
        slots_ref[:, cols] = jnp.dot(
            select_ref[...], normed, preferred_element_type=jnp.float32
        ).astype(jnp.bfloat16)

    def drain_q(d, carry):
        q_copy(d).wait_send()
        return carry

    lax.fori_loop(1, N_SP, drain_q, 0)

    def drain_heads(g, carry):
        @pl.when(jnp.logical_or(g != sp, sp != tp))
        def _():
            head_copy(g, tp).wait_send()

        return carry

    lax.fori_loop(0, N_SP, drain_heads, 0)
    for half in range(2):
        for index in range(20):
            part = None if index in (0, 1) or 4 <= index < 12 else 0
            kv_copy(half, index, sp, part, 1, 0).wait_send()


def attend(q, kv, w, lam, gain, select, residual, norm_gain):
    anywhere = pl.BlockSpec(memory_space=pl.ANY)
    vmem = pl.BlockSpec(memory_space=pltpu.VMEM)
    smem = pl.BlockSpec(memory_space=pltpu.SMEM)
    dma = pltpu.SemaphoreType.DMA
    return pl.pallas_call(
        attend_kernel,
        out_shape=(
            jax.ShapeDtypeStruct((ROWS, DEPTH), jnp.bfloat16),
            jax.ShapeDtypeStruct((SLOTS, DEPTH), jnp.bfloat16),
        ),
        in_specs=[anywhere, anywhere, anywhere, smem, vmem, vmem, vmem, vmem],
        out_specs=(vmem, vmem),
        scratch_shapes=[
            pltpu.VMEM((N_SP, ROWS, LANES), jnp.bfloat16),
            pltpu.VMEM((N_SP, ROWS, LANES), jnp.bfloat16),
            pltpu.VMEM((N_SP, GROUP, LANES), jnp.bfloat16),
            pltpu.VMEM((N_SP, 2, 2, HALF, LANES), jnp.bfloat16),
            pltpu.VMEM((N_SP * GROUP, 2 * LANES), jnp.float32),
            pltpu.VMEM((N_SP * GROUP, LANES), jnp.float32),
            pltpu.VMEM((N_SP, ROWS, LANES), jnp.bfloat16),
            pltpu.VMEM((ROWS, DEPTH), jnp.bfloat16),
            pltpu.VMEM((DEPTH, DEPTH), jnp.bfloat16),
            dma((3,)),
            dma((N_SP,)),
            dma((N_SP,)),
            dma((2, 20)),
            dma((2, 20)),
            dma((N_SP,)),
            dma((N_TP,)),
        ],
        compiler_params=pltpu.CompilerParams(
            collective_id=0, has_side_effects=True, vmem_limit_bytes=56 * 1024 * 1024
        ),
        name="attend",
    )(q, kv, w, lam, gain, select, residual, norm_gain)


def side_sum(parts, axes, turns):
    shape = [lax.axis_size(a) for a in axes]
    parts = parts.reshape(*shape, *parts.shape[1:])
    parts = parts.transpose(*turns, *range(len(axes), parts.ndim))
    parts = parts.reshape(-1, *parts.shape[len(axes) :])
    for k in turns:
        parts = lax.psum_scatter(parts, axes[k], scatter_dimension=0, tiled=True)
    return parts[0]


def shards(
    queries, key_pairs, head_values, lambdas, head_gain, out_weight, residual, norm_gain,
    expert_ids, route_weights, gate_weight, up_weight, down_weight,
):
    q = queries.reshape(N_SP, ROWS, LANES)
    kv = jnp.stack(
        [key_pairs.reshape(2, HALF, LANES), head_values.reshape(2, HALF, LANES)], axis=1
    )
    flat_ids = expert_ids.reshape(-1)
    routes = flat_ids.shape[0]
    same = flat_ids[:, None] == flat_ids[None, :]
    earlier = jnp.arange(routes)[:, None] > jnp.arange(routes)[None, :]
    ranking = jnp.sum((same & earlier).astype(jnp.int32), axis=1)
    slots = (flat_ids * CAP + ranking).reshape(ROWS, 2)
    hit = slots[:, :, None] == jnp.arange(SLOTS, dtype=jnp.int32)[None, None, :]
    select = jnp.any(hit, axis=1).T.astype(jnp.bfloat16)
    updated, outgoing = attend(
        q, kv, out_weight, lambdas.reshape(1, 1), head_gain.reshape(1, LANES), select,
        residual, norm_gain.reshape(1, DEPTH),
    )
    arrived = lax.all_to_all(
        outgoing.reshape(N_SP, 2, CAP, DEPTH), "sp", split_axis=0, concat_axis=0, tiled=True
    )
    piece_rows = lax.all_gather(arrived[None], "tp", axis=0, tiled=True)
    gate_part = jnp.einsum(
        "tsecd,edf->tsecf", piece_rows, gate_weight, preferred_element_type=jnp.float32
    )
    up_part = jnp.einsum(
        "tsecd,edf->tsecf", piece_rows, up_weight, preferred_element_type=jnp.float32
    )
    inner_rows = (jax.nn.silu(gate_part) * up_part).astype(jnp.bfloat16)
    partial_value = jnp.einsum(
        "tsecf,efd->tsecd", inner_rows, down_weight, preferred_element_type=jnp.float32
    )
    reduced = lax.psum_scatter(
        partial_value.astype(jnp.bfloat16), "tp", scatter_dimension=0, tiled=True
    )
    returned = lax.all_to_all(reduced[0], "sp", split_axis=0, concat_axis=0, tiled=True)
    weight = jnp.sum(jnp.where(hit, route_weights[:, :, None], 0.0), axis=1)
    moe_sum = jnp.dot(
        weight, returned.reshape(SLOTS, DEPTH).astype(jnp.float32), precision=lax.Precision.HIGHEST
    )
    return (updated.astype(jnp.float32) + moe_sum).astype(jnp.bfloat16)


def solution(mesh):
    in_specs = (
        P("sp", "tp", None),
        P("sp", "tp", None),
        P("sp", "tp", None),
        P("tp"),
        P(),
        P(),
        P(("sp", "tp"), None),
        P(),
        P(("sp", "tp"), None),
        P(("sp", "tp"), None),
        P("sp", None, "tp"),
        P("sp", None, "tp"),
        P("sp", "tp", None),
    )
    return jax.shard_map(
        shards, mesh=mesh, in_specs=in_specs, out_specs=P(("sp", "tp"), None), check_vma=False
    )
```

```python
import functools

import jax
import jax.numpy as jnp
from jax import lax
from jax.experimental import pallas as pl
from jax.experimental.pallas import tpu as pltpu
from jax.sharding import PartitionSpec as P

MESH = pl.DeviceIdType.MESH
SIDE = 4
N_SP = 16
N_TP = 16
ROWS = 48
SPAN = N_TP * ROWS
HALF = SPAN // 2
GROUP = 2 * ROWS
TILE_GROUPS = 4
TILE = TILE_GROUPS * GROUP
LANES = 128
HD = 64
DEPTH = 2048
EXPERTS = 32
CAP = 4
SLOTS = EXPERTS * CAP
COLS = 512
NEG = -1e30

ORDER = [
    (0, 0), (-1, 0), (1, 0), (0, -1), (0, 1), (2, 0), (-1, -1), (-1, 1),
    (1, -1), (1, 1), (2, -1), (2, 1), (0, 2), (-1, 2), (1, 2), (2, 2),
]
PLACE = {0: 0, -1: 1, 1: 2, 2: 3}


def pick(index, values):
    out = jnp.int32(values[0])
    for k, value in enumerate(values):
        out = jnp.where(index == k, jnp.int32(value), out)
    return out


def mod(value, size):
    return lax.rem(value + size, size)


def attend_kernel(
    q_hbm, kv_hbm, w_hbm, lam_ref, gain_ref, select_ref, residual_ref, norm_gain_ref,
    updated_ref, slots_ref,
    q_own, q_land, qs, kvb, acc, top, own_heads, heads, w_vmem,
    local_sem, q_send, q_recv, kv_send, kv_recv, head_send, head_recv,
):
    sp = lax.axis_index("sp")
    tp = lax.axis_index("tp")
    x, y = lax.rem(sp, SIDE), sp // SIDE

    barrier = pltpu.get_barrier_semaphore()
    load_w = pltpu.make_async_copy(w_hbm, w_vmem, local_sem.at[0])
    load_w.start()
    load_kv = pltpu.make_async_copy(kv_hbm, kvb.at[sp], local_sem.at[1])
    load_kv.start()
    load_q = pltpu.make_async_copy(q_hbm, q_own, local_sem.at[2])
    load_q.start()

    def greet_plane(d, carry):
        pl.semaphore_signal(
            barrier, inc=1, device_id=(lax.rem(sp + d, N_SP), tp), device_id_type=MESH
        )
        return carry

    lax.fori_loop(1, N_SP, greet_plane, 0)

    def greet_sources(h, carry):
        @pl.when(jnp.logical_or(tp != sp, h != tp))
        def _():
            pl.semaphore_signal(barrier, inc=1, device_id=(tp, h), device_id_type=MESH)

        return carry

    lax.fori_loop(0, N_TP, greet_sources, 0)
    pl.semaphore_wait(
        barrier, N_SP - 1 + N_TP - jnp.where(sp == tp, jnp.int32(1), jnp.int32(0))
    )

    load_q.wait()

    def q_copy(d):
        other = lax.rem(sp + d, N_SP)
        return pltpu.make_async_remote_copy(
            src_ref=q_own.at[other], dst_ref=q_land.at[sp],
            send_sem=q_send.at[d], recv_sem=q_recv.at[d],
            device_id=(other, tp), device_id_type=MESH,
        )

    def send_q(d, carry):
        q_copy(d).start()
        return carry

    lax.fori_loop(1, N_SP, send_q, 0)
    load_kv.wait()

    def block_of(half, du, dv):
        dx, dy = (du, dv) if half == 0 else (dv, du)
        return mod(y + dy, SIDE) * SIDE + mod(x + dx, SIDE)

    def kv_copy(half, index, block, part, du, dv):
        ref = kvb.at[block, half] if part is None else kvb.at[block, half, part]
        return pltpu.make_async_remote_copy(
            src_ref=ref, dst_ref=ref,
            send_sem=kv_send.at[half, index], recv_sem=kv_recv.at[half, index],
            device_id=(block_of(half, du, dv), tp), device_id_type=MESH,
        )

    def send(half, index, rel, part, du, dv):
        kv_copy(half, index, block_of(half, *rel), part, du, dv).start()

    def arrived(half, index, rel, part):
        kv_copy(half, index, block_of(half, *rel), part, 1, 0).wait_recv()

    for half in range(2):
        send(half, 0, (0, 0), None, 1, 0)
        send(half, 1, (0, 0), None, -1, 0)
        send(half, 4, (0, 0), None, 0, 1)
        send(half, 8, (0, 0), None, 0, -1)

    for own in range(N_SP):
        @pl.when(sp == own)
        def _():
            q_land[own] = q_own[own]

    lane = lax.broadcasted_iota(jnp.int32, (ROWS, LANES), 1)

    def wait_q(d, carry):
        q_copy(d).wait_recv()
        return carry

    lax.fori_loop(1, N_SP, wait_q, 0)

    def pack_q(g, carry):
        rows = q_land[g].astype(jnp.float32) * (HD**-0.5)
        qs[g, 0:ROWS] = jnp.where(lane < HD, rows, 0.0).astype(jnp.bfloat16)
        qs[g, ROWS:GROUP] = jnp.where(lane >= HD, rows, 0.0).astype(jnp.bfloat16)
        return carry

    lax.fori_loop(0, N_SP, pack_q, 0)
    acc[...] = jnp.zeros_like(acc)
    top[...] = jnp.full_like(top, NEG)

    row = lax.broadcasted_iota(jnp.int32, (TILE_GROUPS, GROUP, HALF), 1)
    row = jnp.where(row >= ROWS, row - ROWS, row)
    offset = (
        lax.broadcasted_iota(jnp.int32, (TILE_GROUPS, GROUP, HALF), 0) * SPAN
        + row
        - lax.broadcasted_iota(jnp.int32, (TILE_GROUPS, GROUP, HALF), 2)
    ).reshape(TILE, HALF)

    def tile_step(t, block, half, masked):
        rows = pl.ds(pl.multiple_of(t * TILE, TILE), TILE)
        q_tile = qs[pl.ds(t * TILE_GROUPS, TILE_GROUPS)].reshape(TILE, LANES)
        keys = kvb[block, half, 0]
        values = kvb[block, half, 1]
        scores = lax.dot_general(
            q_tile, keys, (((1,), (1,)), ((), ())), preferred_element_type=jnp.float32
        )
        if masked:
            ahead = block * SPAN + half * HALF - t * (TILE_GROUPS * SPAN) - sp * ROWS
            scores = jnp.where(offset >= ahead, scores, -jnp.inf)
        old_top = top[rows]
        new_top = jnp.maximum(old_top, jnp.max(scores, axis=1, keepdims=True))
        decay = jnp.exp(old_top - new_top)
        weights = jnp.exp(scores - new_top[:, 0:1]).astype(jnp.bfloat16)
        wide = jnp.concatenate([values, jnp.ones_like(values)], axis=1)
        fresh = jnp.dot(weights, wide, preferred_element_type=jnp.float32)
        acc[rows] = acc[rows] * jnp.concatenate([decay, decay], axis=1) + fresh
        top[rows] = new_top

    def use_block(block, half):
        first = block // TILE_GROUPS
        tile_step(first, block, half, True)

        def later(t, carry):
            tile_step(t, block, half, False)
            return carry

        lax.fori_loop(first + 1, N_SP // TILE_GROUPS, later, 0)

    def step(s, carry):
        def on(k, half):
            du, dv = ORDER[k]
            if k == 1:
                arrived(half, 0, (-1, 0), None)
                send(half, 2, (-1, 0), 0, 1, 0)
                send(half, 5, (-1, 0), None, 0, 1)
                send(half, 9, (-1, 0), None, 0, -1)
            elif k == 2:
                arrived(half, 1, (1, 0), None)
                send(half, 3, (1, 0), 1, -1, 0)
                send(half, 6, (1, 0), None, 0, 1)
                send(half, 10, (1, 0), None, 0, -1)
            elif k == 5:
                arrived(half, 2, (2, 0), 0)
                arrived(half, 3, (2, 0), 1)
                send(half, 7, (2, 0), None, 0, 1)
                send(half, 11, (2, 0), None, 0, -1)
            elif dv == -1:
                place = PLACE[du]
                arrived(half, 4 + place, (du, dv), None)
                send(half, 12 + place, (du, dv), 0, 0, 1)
            elif dv == 1:
                place = PLACE[du]
                arrived(half, 8 + place, (du, dv), None)
                send(half, 16 + place, (du, dv), 1, 0, -1)
            elif dv == 2:
                place = PLACE[du]
                arrived(half, 12 + place, (du, dv), 0)
                arrived(half, 16 + place, (du, dv), 1)

        for k in range(1, len(ORDER)):
            @pl.when(s == k)
            def _():
                for half in range(2):
                    on(k, half)

        du = pick(s, [o[0] for o in ORDER])
        dv = pick(s, [o[1] for o in ORDER])

        def one_half(half, carry):
            dx = jnp.where(half == 0, du, dv)
            dy = jnp.where(half == 0, dv, du)
            block = mod(y + dy, SIDE) * SIDE + mod(x + dx, SIDE)
            use_block(block, half)
            return carry

        return lax.fori_loop(0, 2, one_half, carry)

    lax.fori_loop(0, len(ORDER), step, 0)

    lam = lam_ref[0, 0]

    def finish(g, carry):
        part = acc[pl.ds(pl.multiple_of(g * GROUP, GROUP), GROUP)]
        ratio = part[:, 0:LANES] / part[:, LANES : 2 * LANES]
        mixed = ratio[0:ROWS] - lam * ratio[ROWS:GROUP]
        square = jnp.mean(mixed * mixed, axis=1, keepdims=True)
        own_heads[g] = (mixed * lax.rsqrt(square + 1e-06) * gain_ref[...]).astype(
            jnp.bfloat16
        )
        return carry

    lax.fori_loop(0, N_SP, finish, 0)

    def head_copy(g, h):
        return pltpu.make_async_remote_copy(
            src_ref=own_heads.at[g],
            dst_ref=heads.at[:, pl.ds(pl.multiple_of(tp * LANES, LANES), LANES)],
            send_sem=head_send.at[g], recv_sem=head_recv.at[h],
            device_id=(g, sp), device_id_type=MESH,
        )

    def push_head(g, carry):
        @pl.when(jnp.logical_or(g != sp, sp != tp))
        def _():
            head_copy(g, tp).start()

        return carry

    lax.fori_loop(0, N_SP, push_head, 0)

    for own in range(N_SP):
        @pl.when(jnp.logical_and(sp == own, tp == own))
        def _():
            heads[:, own * LANES : (own + 1) * LANES] = own_heads[own]

    load_w.wait()

    def wait_head(h, carry):
        @pl.when(jnp.logical_or(h != tp, sp != tp))
        def _():
            head_copy(0, h).wait_recv()

        return carry

    lax.fori_loop(0, N_TP, wait_head, 0)

    attended = heads[...]
    squares = jnp.zeros((ROWS, 1), jnp.float32)
    wide = []
    for n in range(DEPTH // COLS):
        cols = slice(n * COLS, (n + 1) * COLS)
        projected = jnp.dot(attended, w_vmem[:, cols], preferred_element_type=jnp.float32)
        updated = (residual_ref[:, cols].astype(jnp.float32) + projected).astype(jnp.bfloat16)
        updated_ref[:, cols] = updated
        back = updated.astype(jnp.float32)
        squares = squares + jnp.sum(back * back, axis=1, keepdims=True)
        wide.append(back)
    scale = lax.rsqrt(squares / DEPTH + 1e-06)
    for n in range(DEPTH // COLS):
        cols = slice(n * COLS, (n + 1) * COLS)
        normed = (wide[n] * scale * norm_gain_ref[:, cols]).astype(jnp.bfloat16)
        packed = jnp.dot(select_ref[...], normed, preferred_element_type=jnp.float32)
        slots_ref[:, :, cols] = packed.reshape(N_SP, 8, COLS).astype(jnp.bfloat16)

    def drain_q(d, carry):
        q_copy(d).wait_send()
        return carry

    lax.fori_loop(1, N_SP, drain_q, 0)

    def drain_heads(g, carry):
        @pl.when(jnp.logical_or(g != sp, sp != tp))
        def _():
            head_copy(g, tp).wait_send()

        return carry

    lax.fori_loop(0, N_SP, drain_heads, 0)
    for half in range(2):
        for index in range(20):
            part = None if index in (0, 1) or 4 <= index < 12 else 0
            kv_copy(half, index, sp, part, 1, 0).wait_send()


def attend(q, kv, w, lam, gain, select, residual, norm_gain):
    anywhere = pl.BlockSpec(memory_space=pl.ANY)
    vmem = pl.BlockSpec(memory_space=pltpu.VMEM)
    smem = pl.BlockSpec(memory_space=pltpu.SMEM)
    dma = pltpu.SemaphoreType.DMA
    return pl.pallas_call(
        attend_kernel,
        out_shape=(
            jax.ShapeDtypeStruct((ROWS, DEPTH), jnp.bfloat16),
            jax.ShapeDtypeStruct((N_SP, 8, DEPTH), jnp.bfloat16),
        ),
        in_specs=[anywhere, anywhere, anywhere, smem, vmem, vmem, vmem, vmem],
        out_specs=(vmem, vmem),
        scratch_shapes=[
            pltpu.VMEM((N_SP, ROWS, LANES), jnp.bfloat16),
            pltpu.VMEM((N_SP, ROWS, LANES), jnp.bfloat16),
            pltpu.VMEM((N_SP, GROUP, LANES), jnp.bfloat16),
            pltpu.VMEM((N_SP, 2, 2, HALF, LANES), jnp.bfloat16),
            pltpu.VMEM((N_SP * GROUP, 2 * LANES), jnp.float32),
            pltpu.VMEM((N_SP * GROUP, LANES), jnp.float32),
            pltpu.VMEM((N_SP, ROWS, LANES), jnp.bfloat16),
            pltpu.VMEM((ROWS, DEPTH), jnp.bfloat16),
            pltpu.VMEM((DEPTH, DEPTH), jnp.bfloat16),
            dma((3,)),
            dma((N_SP,)),
            dma((N_SP,)),
            dma((2, 20)),
            dma((2, 20)),
            dma((N_SP,)),
            dma((N_TP,)),
        ],
        compiler_params=pltpu.CompilerParams(
            collective_id=0, has_side_effects=True, vmem_limit_bytes=56 * 1024 * 1024
        ),
        name="attend",
    )(q, kv, w, lam, gain, select, residual, norm_gain)


RING = 8
PIECE = 8
WIDE = 2 * LANES
MID = DEPTH // 2
Z_ORDER = [0, -1, 1, -2, 2, -3, 3, 4]
Z_PLACE = {d: k for k, d in enumerate(Z_ORDER)}


def expert_kernel(
    slots_hbm, gate_hbm, up_hbm, down_hbm, comb_hbm, updated_ref,
    merged_ref,
    slots_own, rows, gate_up, down, comb_own, comb, own_part, pair_out, pair_in, out,
    res, red, sum_out, sum_in,
    local_sem, slot_send, slot_recv, ring_send, ring_recv, fwd_send, fwd_recv,
    pair_send, pair_recv, res_send, res_recv, comb_send, comb_recv, sum_send, sum_recv,
):
    sp = lax.axis_index("sp")
    tp = lax.axis_index("tp")
    z, core = tp // 2, lax.rem(tp, 2)

    barrier = pltpu.get_barrier_semaphore()

    def load(k, src, dst):
        return pltpu.make_async_copy(src, dst, local_sem.at[k])

    loads = [
        load(0, slots_hbm, slots_own),
        load(1, slots_hbm.at[sp], rows.at[tp, sp]),
        load(2, comb_hbm, comb_own),
        load(3, comb_hbm, comb.at[z]),
    ]
    for e in range(2):
        loads += [
            load(4 + e, gate_hbm.at[e], gate_up.at[:, e * LANES : (e + 1) * LANES]),
            load(6 + e, up_hbm.at[e], gate_up.at[:, (2 + e) * LANES : (3 + e) * LANES]),
            load(8 + e, down_hbm.at[e], down.at[e * LANES : (e + 1) * LANES]),
        ]
    for item in loads:
        item.start()

    def greet_plane(d, carry):
        pl.semaphore_signal(
            barrier, inc=1, device_id=(lax.rem(sp + d, N_SP), tp), device_id_type=MESH
        )
        return carry

    lax.fori_loop(1, N_SP, greet_plane, 0)

    def at_z(dz):
        return (sp, 2 * mod(z + dz, RING) + core)

    def greet_ring(d, carry):
        pl.semaphore_signal(barrier, inc=1, device_id=at_z(d), device_id_type=MESH)
        return carry

    lax.fori_loop(1, RING, greet_ring, 0)
    partner = (sp, 2 * z + (1 - core))
    pl.semaphore_signal(barrier, inc=1, device_id=partner, device_id_type=MESH)
    pl.semaphore_wait(barrier, N_SP - 1 + RING - 1 + 1)

    def remote(src, dst, send_sem, recv_sem, device):
        return pltpu.make_async_remote_copy(
            src_ref=src, dst_ref=dst, send_sem=send_sem, recv_sem=recv_sem,
            device_id=device, device_id_type=MESH,
        )

    def slot_copy(d):
        other = lax.rem(sp + d, N_SP)
        return remote(
            slots_own.at[other], rows.at[tp, sp], slot_send.at[d], slot_recv.at[d], (other, tp)
        )

    loads[0].wait()

    def send_slot(d, carry):
        slot_copy(d).start()
        return carry

    lax.fori_loop(1, N_SP, send_slot, 0)
    loads[2].wait()

    def comb_copy(d):
        return remote(comb_own, comb.at[z], comb_send.at[d], comb_recv.at[d], at_z(d))

    def send_comb(d, carry):
        comb_copy(d).start()
        return carry

    lax.fori_loop(1, RING, send_comb, 0)
    for item in loads[1:2] + loads[3:]:
        item.wait()

    def ring_copy(way, m, dz, piece):
        ref = rows.at[2 * mod(z + dz, RING) + core, pl.ds(piece * PIECE, PIECE)]
        return remote(
            ref, ref, ring_send.at[way, m], ring_recv.at[way, m], at_z(1 if way == 0 else -1)
        )

    def fwd_copy(j, dz):
        ref = rows.at[2 * mod(z + dz, RING) + core]
        return remote(ref, ref, fwd_send.at[j], fwd_recv.at[j], partner)

    def pair_copy(j):
        return remote(pair_out.at[j], pair_in.at[j], pair_send.at[j], pair_recv.at[j], partner)

    def res_copy(j, d):
        other = lax.rem(sp + d, N_SP)
        return remote(
            out.at[j, other], res.at[j, sp], res_send.at[j, d], res_recv.at[j, d], (other, tp)
        )

    def ring_event(k):
        if k == 0:
            for piece in range(2):
                def wait_slot(src, carry):
                    d = mod(sp - src, N_SP)

                    @pl.when(d != 0)
                    def _():
                        slot_copy(d).wait_recv()

                    return carry

                lax.fori_loop(piece * PIECE, (piece + 1) * PIECE, wait_slot, 0)
                for way in range(2):
                    ring_copy(way, piece, 0, piece).start()
            fwd_copy(0, 0).start()
        elif k < 4:
            for piece in range(2):
                for way in range(2):
                    dz = -k if way == 0 else k
                    ring_copy(way, 2 * (k - 1) + piece, dz, piece).wait_recv()
                    if k < 3:
                        ring_copy(way, 2 * k + piece, dz, piece).start()
                    elif piece == way:
                        ring_copy(way, 6, dz, piece).start()
            fwd_copy(2 * k - 1, -k).start()
            fwd_copy(2 * k, k).start()
        else:
            ring_copy(0, 6, 4, 0).wait_recv()
            ring_copy(1, 6, 4, 1).wait_recv()
            fwd_copy(7, 4).start()

    row_expert = lax.rem(lax.broadcasted_iota(jnp.int32, (2 * N_SP * CAP, WIDE), 0), 8) // CAP
    col_expert = lax.broadcasted_iota(jnp.int32, (2 * N_SP * CAP, WIDE), 1) // LANES
    mine = row_expert == col_expert

    def chunk_part(chunk, dst, j):
        x = rows[chunk].reshape(2 * N_SP * CAP, DEPTH)
        gate = jnp.dot(x, gate_up[:, 0:WIDE], preferred_element_type=jnp.float32)
        up = jnp.dot(x, gate_up[:, WIDE : 2 * WIDE], preferred_element_type=jnp.float32)
        inner = gate / (1.0 + jnp.exp(-gate)) * up
        inner = jnp.where(mine, inner, 0.0).astype(jnp.bfloat16)
        for n in range(DEPTH // COLS):
            cols = slice(n * COLS, (n + 1) * COLS)
            piece = jnp.dot(inner, down[:, cols], preferred_element_type=jnp.float32)
            dst[j, :, :, cols] = piece.reshape(N_SP, 8, COLS).astype(jnp.bfloat16)

    def push_results(j):
        pair_copy(j).wait_recv()
        total = own_part[j].astype(jnp.float32) + pair_in[j].astype(jnp.float32)
        out[j] = total.astype(jnp.bfloat16)
        res[j, sp] = out[j, sp]

        def push(d, carry):
            res_copy(j, d).start()
            return carry

        lax.fori_loop(1, N_SP, push, 0)

    def combine(j):
        def wait_res(d, carry):
            res_copy(j, d).wait_recv()
            return carry

        lax.fori_loop(1, N_SP, wait_res, 0)
        zj = mod(z + pick(j, Z_ORDER), RING)

        @pl.when(zj != z)
        def _():
            comb_copy(mod(z - zj, RING)).wait_recv()

        high, low = comb[zj, :, 0:LANES], comb[zj, :, LANES:WIDE]
        for n in range(DEPTH // COLS):
            cols = slice(n * COLS, (n + 1) * COLS)
            found = res[j, :, :, cols].reshape(SLOTS, COLS)
            red[j, :, cols] = jnp.dot(
                high, found, preferred_element_type=jnp.float32
            ) + jnp.dot(low, found, preferred_element_type=jnp.float32)

    def step(j, carry):
        for k, at in enumerate((0, 1, 3, 5, 7)):
            @pl.when(j == at)
            def _():
                ring_event(k)

        zj = mod(z + pick(j, Z_ORDER), RING)
        chunk_part(2 * zj + core, own_part, j)
        fwd_copy(j, 0).wait_recv()
        chunk_part(2 * zj + (1 - core), pair_out, j)
        pair_copy(j).start()

        @pl.when(j >= 1)
        def _():
            push_results(j - 1)

        @pl.when(j >= 3)
        def _():
            combine(j - 3)

        return carry

    lax.fori_loop(0, RING, step, 0)
    push_results(RING - 1)

    def late(j, carry):
        combine(j)
        return carry

    lax.fori_loop(RING - 3, RING, late, 0)

    def sum_copy(way, r, h):
        cols = slice(h * MID, (h + 1) * MID)
        return remote(
            sum_out.at[way, r, :, cols], sum_in.at[way, r, :, cols],
            sum_send.at[way, r, h], sum_recv.at[way, r, h], at_z(-1 if way == 0 else 1),
        )

    def sum_step(way, r, h):
        cols = slice(h * MID, (h + 1) * MID)
        d = 4 if r == 0 else (r - 4 if way == 0 else 4 - r)
        value = red[Z_PLACE[d], :, cols]
        if r > 1 or (r == 1 and h == way):
            sum_copy(way, r - 1, h).wait_recv()
            value = value + sum_in[way, r - 1, :, cols].astype(jnp.float32)
        sum_out[way, r, :, cols] = value.astype(jnp.bfloat16)
        sum_copy(way, r, h).start()

    sum_step(0, 0, 0)
    sum_step(1, 0, 1)
    for r in range(1, 4):
        sum_step(0, r, 1)
        sum_step(1, r, 0)
        sum_step(0, r, 0)
        sum_step(1, r, 1)
    for h in range(2):
        cols = slice(h * MID, (h + 1) * MID)
        total = updated_ref[:, cols].astype(jnp.float32) + red[0, :, cols]
        for way in range(2):
            sum_copy(way, 3, h).wait_recv()
            total = total + sum_in[way, 3, :, cols].astype(jnp.float32)
        merged_ref[:, cols] = total.astype(jnp.bfloat16)

    def drain_plane(d, carry):
        slot_copy(d).wait_send()

        def drain_res(j, inner):
            res_copy(j, d).wait_send()
            return inner

        return lax.fori_loop(0, RING, drain_res, carry)

    lax.fori_loop(1, N_SP, drain_plane, 0)

    def drain_comb(d, carry):
        comb_copy(d).wait_send()
        return carry

    lax.fori_loop(1, RING, drain_comb, 0)

    def drain_pair(j, carry):
        fwd_copy(j, 0).wait_send()
        pair_copy(j).wait_send()
        return carry

    lax.fori_loop(0, RING, drain_pair, 0)
    for way in range(2):
        for m in range(7):
            ring_copy(way, m, 0, 0).wait_send()
        for r in range(4):
            for h in range(2):
                if r > 0 or h == way:
                    sum_copy(way, r, h).wait_send()


def experts(slots, gate, up, down, comb, updated):
    anywhere = pl.BlockSpec(memory_space=pl.ANY)
    vmem = pl.BlockSpec(memory_space=pltpu.VMEM)
    dma = pltpu.SemaphoreType.DMA
    chunk = (N_SP, 8, DEPTH)
    bf16, f32 = jnp.bfloat16, jnp.float32
    return pl.pallas_call(
        expert_kernel,
        out_shape=jax.ShapeDtypeStruct((ROWS, DEPTH), bf16),
        in_specs=[anywhere] * 5 + [vmem],
        out_specs=vmem,
        scratch_shapes=[
            pltpu.VMEM(chunk, bf16),
            pltpu.VMEM((N_TP, *chunk), bf16),
            pltpu.VMEM((DEPTH, 2 * WIDE), bf16),
            pltpu.VMEM((WIDE, DEPTH), bf16),
            pltpu.VMEM((ROWS, WIDE), bf16),
            pltpu.VMEM((RING, ROWS, WIDE), bf16),
            pltpu.VMEM((RING, *chunk), bf16),
            pltpu.VMEM((RING, *chunk), bf16),
            pltpu.VMEM((RING, *chunk), bf16),
            pltpu.VMEM((RING, *chunk), bf16),
            pltpu.VMEM((RING, *chunk), bf16),
            pltpu.VMEM((RING, ROWS, DEPTH), f32),
            pltpu.VMEM((2, 4, ROWS, DEPTH), bf16),
            pltpu.VMEM((2, 4, ROWS, DEPTH), bf16),
            dma((10,)),
            dma((N_SP,)),
            dma((N_SP,)),
            dma((2, 7)),
            dma((2, 7)),
            dma((RING,)),
            dma((RING,)),
            dma((RING,)),
            dma((RING,)),
            dma((RING, N_SP)),
            dma((RING, N_SP)),
            dma((RING,)),
            dma((RING,)),
            dma((2, 4, 2)),
            dma((2, 4, 2)),
        ],
        compiler_params=pltpu.CompilerParams(
            collective_id=1, has_side_effects=True, vmem_limit_bytes=56 * 1024 * 1024
        ),
        name="experts",
    )(slots, gate, up, down, comb, updated)


def shards(
    queries, key_pairs, head_values, lambdas, head_gain, out_weight, residual, norm_gain,
    expert_ids, route_weights, gate_weight, up_weight, down_weight,
):
    q = queries.reshape(N_SP, ROWS, LANES)
    kv = jnp.stack(
        [key_pairs.reshape(2, HALF, LANES), head_values.reshape(2, HALF, LANES)], axis=1
    )
    flat_ids = expert_ids.reshape(-1)
    routes = flat_ids.shape[0]
    same = flat_ids[:, None] == flat_ids[None, :]
    earlier = jnp.arange(routes)[:, None] > jnp.arange(routes)[None, :]
    ranking = jnp.sum((same & earlier).astype(jnp.int32), axis=1)
    slots = (flat_ids * CAP + ranking).reshape(ROWS, 2)
    hit = slots[:, :, None] == jnp.arange(SLOTS, dtype=jnp.int32)[None, None, :]
    select = jnp.any(hit, axis=1).T.astype(jnp.bfloat16)
    weight = jnp.sum(jnp.where(hit, route_weights[:, :, None], 0.0), axis=1)
    high = weight.astype(jnp.bfloat16)
    low = (weight - high.astype(jnp.float32)).astype(jnp.bfloat16)
    updated, outgoing = attend(
        q, kv, out_weight, lambdas.reshape(1, 1), head_gain.reshape(1, LANES), select,
        residual, norm_gain.reshape(1, DEPTH),
    )
    return experts(
        outgoing, gate_weight, up_weight, down_weight, jnp.concatenate([high, low], axis=1),
        updated,
    )


def solution(mesh):
    in_specs = (
        P("sp", "tp", None),
        P("sp", "tp", None),
        P("sp", "tp", None),
        P("tp"),
        P(),
        P(),
        P(("sp", "tp"), None),
        P(),
        P(("sp", "tp"), None),
        P(("sp", "tp"), None),
        P("sp", None, "tp"),
        P("sp", None, "tp"),
        P("sp", "tp", None),
    )
    return jax.shard_map(
        shards, mesh=mesh, in_specs=in_specs, out_specs=P(("sp", "tp"), None), check_vma=False
    )
```

```python
import functools

import jax
import jax.numpy as jnp
from jax import lax
from jax.experimental import pallas as pl
from jax.experimental.pallas import tpu as pltpu
from jax.sharding import PartitionSpec as P

MESH = pl.DeviceIdType.MESH
SIDE = 4
N_SP = 16
N_TP = 16
ROWS = 48
SPAN = N_TP * ROWS
HALF = SPAN // 2
LANES = 128
TILES = SPAN // LANES
ONES = 16
HD = 64
DEPTH = 2048
EXPERTS = 32
CAP = 4
SLOTS = EXPERTS * CAP
COLS = 512
NEG = -1e30

ORDER = [
    (0, 0), (-1, 0), (1, 0), (0, -1), (0, 1), (2, 0), (-1, -1), (-1, 1),
    (1, -1), (1, 1), (2, -1), (2, 1), (0, 2), (-1, 2), (1, 2), (2, 2),
]
PLACE = {0: 0, -1: 1, 1: 2, 2: 3}


def pick(index, values):
    out = jnp.int32(values[0])
    for k, value in enumerate(values):
        out = jnp.where(index == k, jnp.int32(value), out)
    return out


def mod(value, size):
    return lax.rem(value + size, size)


def attend_kernel(
    q_hbm, kv_hbm, w_hbm, lam_ref, gain_ref, select_ref, residual_ref, norm_gain_ref,
    updated_ref, slots_ref,
    q_own, q_land, qs, kvb, acc, top, score_a, score_b, weight_a, weight_b,
    own_heads, heads, w_vmem,
    local_sem, q_send, q_recv, kv_send, kv_recv, head_send, head_recv,
):
    sp = lax.axis_index("sp")
    tp = lax.axis_index("tp")
    x, y = lax.rem(sp, SIDE), sp // SIDE

    barrier = pltpu.get_barrier_semaphore()
    load_w = pltpu.make_async_copy(w_hbm, w_vmem, local_sem.at[0])
    load_w.start()
    load_kv = pltpu.make_async_copy(kv_hbm, kvb.at[sp], local_sem.at[1])
    load_kv.start()
    load_q = pltpu.make_async_copy(q_hbm, q_own, local_sem.at[2])
    load_q.start()

    def greet_plane(d, carry):
        pl.semaphore_signal(
            barrier, inc=1, device_id=(lax.rem(sp + d, N_SP), tp), device_id_type=MESH
        )
        return carry

    lax.fori_loop(1, N_SP, greet_plane, 0)

    def owner(i, b):
        return lax.rem(i + b, N_TP)

    source = mod(tp - sp, N_SP)
    keeps = owner(sp, sp) == tp

    def greet_sources(h, carry):
        @pl.when(jnp.logical_or(jnp.logical_not(keeps), h != tp))
        def _():
            pl.semaphore_signal(barrier, inc=1, device_id=(source, h), device_id_type=MESH)

        return carry

    lax.fori_loop(0, N_TP, greet_sources, 0)
    pl.semaphore_wait(
        barrier, N_SP - 1 + N_TP - jnp.where(keeps, jnp.int32(1), jnp.int32(0))
    )

    load_q.wait()

    def row_block(g):
        return pl.ds(pl.multiple_of(g * ROWS, ROWS), ROWS)

    def q_copy(d):
        other = lax.rem(sp + d, N_SP)
        return pltpu.make_async_remote_copy(
            src_ref=q_own.at[owner(other, sp)], dst_ref=q_land.at[row_block(sp)],
            send_sem=q_send.at[d], recv_sem=q_recv.at[d],
            device_id=(other, tp), device_id_type=MESH,
        )

    def send_q(d, carry):
        q_copy(d).start()
        return carry

    lax.fori_loop(1, N_SP, send_q, 0)
    load_kv.wait()

    def block_of(half, du, dv):
        dx, dy = (du, dv) if half == 0 else (dv, du)
        return mod(y + dy, SIDE) * SIDE + mod(x + dx, SIDE)

    def kv_copy(half, index, block, part, du, dv):
        ref = kvb.at[block, half] if part is None else kvb.at[block, half, part]
        return pltpu.make_async_remote_copy(
            src_ref=ref, dst_ref=ref,
            send_sem=kv_send.at[half, index], recv_sem=kv_recv.at[half, index],
            device_id=(block_of(half, du, dv), tp), device_id_type=MESH,
        )

    def send(half, index, rel, part, du, dv):
        kv_copy(half, index, block_of(half, *rel), part, du, dv).start()

    def arrived(half, index, rel, part):
        kv_copy(half, index, block_of(half, *rel), part, 1, 0).wait_recv()

    for half in range(2):
        send(half, 0, (0, 0), None, 1, 0)
        send(half, 1, (0, 0), None, -1, 0)
        send(half, 4, (0, 0), None, 0, 1)
        send(half, 8, (0, 0), None, 0, -1)

    for own in range(N_SP):
        @pl.when(sp == own)
        def _():
            q_land[own * ROWS : (own + 1) * ROWS] = q_own[2 * own % N_TP]

    def wait_q(d, carry):
        q_copy(d).wait_recv()
        return carry

    lax.fori_loop(1, N_SP, wait_q, 0)

    lane = lax.broadcasted_iota(jnp.int32, (LANES, LANES), 1)
    for i in range(TILES):
        wide = q_land[i * LANES : (i + 1) * LANES].astype(jnp.float32) * (HD**-0.5)
        qs[i, 0:LANES] = jnp.where(lane < HD, wide, 0.0).astype(jnp.bfloat16)
        qs[i, LANES : 2 * LANES] = jnp.where(lane >= HD, wide, 0.0).astype(jnp.bfloat16)
    acc[...] = jnp.zeros_like(acc)
    top[...] = jnp.full_like(top, NEG)

    score_bufs, weight_bufs = (score_a, score_b), (weight_a, weight_b)

    def tiles_step(first, block, half):
        keys = kvb[block, half, 0]
        wide = jnp.concatenate(
            [kvb[block, half, 1, k * LANES : (k + 1) * LANES] for k in range(HALF // LANES)],
            axis=1,
        )
        wide = jnp.concatenate([wide, jnp.ones((ONES, HALF), jnp.bfloat16)], axis=0)

        def score(i):
            scores = lax.dot_general(
                keys, qs[i], (((1,), (1,)), ((), ())), preferred_element_type=jnp.float32
            )
            if i < first + 3:
                place = lax.broadcasted_iota(jnp.int32, (1, LANES), 1) + i * LANES
                span = lax.shift_right_logical(place * 1366, 16)
                last = (
                    span * (SPAN - ROWS) + place + ((sp + span) & (N_TP - 1)) * ROWS
                    - block * SPAN - half * HALF
                )
                kept = lax.broadcasted_iota(jnp.int32, (HALF, LANES), 0) <= last
                scores = jnp.where(jnp.concatenate([kept, kept], axis=1), scores, -jnp.inf)
            score_bufs[i % 2][...] = scores
            old_top = top[i]
            new_top = jnp.maximum(old_top, jnp.max(scores, axis=0, keepdims=True))
            top[i] = new_top
            return new_top, jnp.exp(old_top - new_top)

        def weigh(i, new_top):
            weights = jnp.exp(score_bufs[i % 2][...] - new_top)
            weight_bufs[i % 2][...] = weights.astype(jnp.bfloat16)

        def add_up(i, decay):
            fresh = jnp.dot(wide, weight_bufs[i % 2][...], preferred_element_type=jnp.float32)
            acc[i] = acc[i] * decay + fresh

        state = {first: score(first)}
        for i in range(first, TILES + 1):
            if i + 1 < TILES:
                state[i + 1] = score(i + 1)
            if i < TILES:
                weigh(i, state[i][0])
            if i > first:
                add_up(i - 1, state[i - 1][1])

    def use_block(block, half):
        first = block * ROWS // LANES // 2
        for k in range(TILES // 2):
            @pl.when(first == k)
            def _():
                tiles_step(2 * k, block, half)

    def step(s, carry):
        def on(k, half):
            du, dv = ORDER[k]
            if k == 1:
                arrived(half, 0, (-1, 0), None)
                send(half, 2, (-1, 0), 0, 1, 0)
                send(half, 5, (-1, 0), None, 0, 1)
                send(half, 9, (-1, 0), None, 0, -1)
            elif k == 2:
                arrived(half, 1, (1, 0), None)
                send(half, 3, (1, 0), 1, -1, 0)
                send(half, 6, (1, 0), None, 0, 1)
                send(half, 10, (1, 0), None, 0, -1)
            elif k == 5:
                arrived(half, 2, (2, 0), 0)
                arrived(half, 3, (2, 0), 1)
                send(half, 7, (2, 0), None, 0, 1)
                send(half, 11, (2, 0), None, 0, -1)
            elif dv == -1:
                place = PLACE[du]
                arrived(half, 4 + place, (du, dv), None)
                send(half, 12 + place, (du, dv), 0, 0, 1)
            elif dv == 1:
                place = PLACE[du]
                arrived(half, 8 + place, (du, dv), None)
                send(half, 16 + place, (du, dv), 1, 0, -1)
            elif dv == 2:
                place = PLACE[du]
                arrived(half, 12 + place, (du, dv), 0)
                arrived(half, 16 + place, (du, dv), 1)

        for k in range(1, len(ORDER)):
            @pl.when(s == k)
            def _():
                for half in range(2):
                    on(k, half)

        du = pick(s, [o[0] for o in ORDER])
        dv = pick(s, [o[1] for o in ORDER])

        def one_half(half, carry):
            dx = jnp.where(half == 0, du, dv)
            dy = jnp.where(half == 0, dv, du)
            block = mod(y + dy, SIDE) * SIDE + mod(x + dx, SIDE)
            use_block(block, half)
            return carry

        return lax.fori_loop(0, 2, one_half, carry)

    lax.fori_loop(0, len(ORDER), step, 0)

    lam = lam_ref[0, 0]

    for i in range(TILES):
        ratio = acc[i, 0:LANES] / acc[i, LANES : LANES + 1]
        mixed = ratio[:, 0:LANES] - lam * ratio[:, LANES : 2 * LANES]
        square = jnp.mean(mixed * mixed, axis=0, keepdims=True)
        done = (mixed * lax.rsqrt(square + 1e-06)).T * gain_ref[...]
        own_heads[i * LANES : (i + 1) * LANES] = done.astype(jnp.bfloat16)

    def head_copy(g, h):
        return pltpu.make_async_remote_copy(
            src_ref=own_heads.at[row_block(g)],
            dst_ref=heads.at[:, pl.ds(pl.multiple_of(tp * LANES, LANES), LANES)],
            send_sem=head_send.at[g], recv_sem=head_recv.at[h],
            device_id=(g, owner(sp, g)), device_id_type=MESH,
        )

    def push_head(g, carry):
        @pl.when(jnp.logical_or(g != sp, jnp.logical_not(keeps)))
        def _():
            head_copy(g, tp).start()

        return carry

    lax.fori_loop(0, N_SP, push_head, 0)

    for own in range(N_SP):
        @pl.when(jnp.logical_and(sp == own, keeps))
        def _():
            at = 2 * own % N_TP * LANES
            heads[:, at : at + LANES] = own_heads[own * ROWS : (own + 1) * ROWS]

    load_w.wait()

    def wait_head(h, carry):
        @pl.when(jnp.logical_or(h != tp, jnp.logical_not(keeps)))
        def _():
            head_copy(0, h).wait_recv()

        return carry

    lax.fori_loop(0, N_TP, wait_head, 0)

    attended = heads[...]
    squares = jnp.zeros((ROWS, 1), jnp.float32)
    wide = []
    for n in range(DEPTH // COLS):
        cols = slice(n * COLS, (n + 1) * COLS)
        projected = jnp.dot(attended, w_vmem[:, cols], preferred_element_type=jnp.float32)
        updated = (residual_ref[:, cols].astype(jnp.float32) + projected).astype(jnp.bfloat16)
        updated_ref[:, cols] = updated
        back = updated.astype(jnp.float32)
        squares = squares + jnp.sum(back * back, axis=1, keepdims=True)
        wide.append(back)
    scale = lax.rsqrt(squares / DEPTH + 1e-06)
    for n in range(DEPTH // COLS):
        cols = slice(n * COLS, (n + 1) * COLS)
        normed = (wide[n] * scale * norm_gain_ref[:, cols]).astype(jnp.bfloat16)
        packed = jnp.dot(select_ref[...], normed, preferred_element_type=jnp.float32)
        slots_ref[:, :, cols] = packed.reshape(N_SP, 8, COLS).astype(jnp.bfloat16)

    def drain_q(d, carry):
        q_copy(d).wait_send()
        return carry

    lax.fori_loop(1, N_SP, drain_q, 0)

    def drain_heads(g, carry):
        @pl.when(jnp.logical_or(g != sp, jnp.logical_not(keeps)))
        def _():
            head_copy(g, tp).wait_send()

        return carry

    lax.fori_loop(0, N_SP, drain_heads, 0)
    for half in range(2):
        for index in range(20):
            part = None if index in (0, 1) or 4 <= index < 12 else 0
            kv_copy(half, index, sp, part, 1, 0).wait_send()


def attend(q, kv, w, lam, gain, select, residual, norm_gain):
    anywhere = pl.BlockSpec(memory_space=pl.ANY)
    vmem = pl.BlockSpec(memory_space=pltpu.VMEM)
    smem = pl.BlockSpec(memory_space=pltpu.SMEM)
    dma = pltpu.SemaphoreType.DMA
    return pl.pallas_call(
        attend_kernel,
        out_shape=(
            jax.ShapeDtypeStruct((ROWS, DEPTH), jnp.bfloat16),
            jax.ShapeDtypeStruct((N_SP, 8, DEPTH), jnp.bfloat16),
        ),
        in_specs=[anywhere, anywhere, anywhere, smem, vmem, vmem, vmem, vmem],
        out_specs=(vmem, vmem),
        scratch_shapes=[
            pltpu.VMEM((N_SP, ROWS, LANES), jnp.bfloat16),
            pltpu.VMEM((SPAN, LANES), jnp.bfloat16),
            pltpu.VMEM((TILES, 2 * LANES, LANES), jnp.bfloat16),
            pltpu.VMEM((N_SP, 2, 2, HALF, LANES), jnp.bfloat16),
            pltpu.VMEM((TILES, LANES + ONES, 2 * LANES), jnp.float32),
            pltpu.VMEM((TILES, 1, 2 * LANES), jnp.float32),
            pltpu.VMEM((HALF, 2 * LANES), jnp.float32),
            pltpu.VMEM((HALF, 2 * LANES), jnp.float32),
            pltpu.VMEM((HALF, 2 * LANES), jnp.bfloat16),
            pltpu.VMEM((HALF, 2 * LANES), jnp.bfloat16),
            pltpu.VMEM((SPAN, LANES), jnp.bfloat16),
            pltpu.VMEM((ROWS, DEPTH), jnp.bfloat16),
            pltpu.VMEM((DEPTH, DEPTH), jnp.bfloat16),
            dma((3,)),
            dma((N_SP,)),
            dma((N_SP,)),
            dma((2, 20)),
            dma((2, 20)),
            dma((N_SP,)),
            dma((N_TP,)),
        ],
        compiler_params=pltpu.CompilerParams(
            collective_id=0, has_side_effects=True, vmem_limit_bytes=56 * 1024 * 1024
        ),
        name="attend",
    )(q, kv, w, lam, gain, select, residual, norm_gain)


RING = 8
PIECE = 8
WIDE = 2 * LANES
PARTS = 4
PART = DEPTH // PARTS
Z_ORDER = [0, -1, 1, -2, 2, -3, 3, 4]
Z_PLACE = {d: k for k, d in enumerate(Z_ORDER)}


def expert_kernel(
    slots_hbm, gate_hbm, up_hbm, down_hbm, comb_hbm, updated_ref,
    merged_ref,
    slots_own, rows, gate_up, down, comb_own, comb, own_part, pair_out, pair_in, out,
    res, red, sum_out, sum_in,
    local_sem, slot_send, slot_recv, ring_send, ring_recv, fwd_send, fwd_recv,
    pair_send, pair_recv, res_send, res_recv, comb_send, comb_recv, sum_send, sum_recv,
):
    sp = lax.axis_index("sp")
    tp = lax.axis_index("tp")
    z, core = tp // 2, lax.rem(tp, 2)

    barrier = pltpu.get_barrier_semaphore()

    def load(k, src, dst):
        return pltpu.make_async_copy(src, dst, local_sem.at[k])

    loads = [
        load(0, slots_hbm, slots_own),
        load(1, slots_hbm.at[sp], rows.at[tp, sp]),
        load(2, comb_hbm, comb_own),
        load(3, comb_hbm, comb.at[z]),
    ]
    for e in range(2):
        loads += [
            load(4 + e, gate_hbm.at[e], gate_up.at[:, e * LANES : (e + 1) * LANES]),
            load(6 + e, up_hbm.at[e], gate_up.at[:, (2 + e) * LANES : (3 + e) * LANES]),
            load(8 + e, down_hbm.at[e], down.at[e * LANES : (e + 1) * LANES]),
        ]
    for item in loads:
        item.start()

    def greet_plane(d, carry):
        pl.semaphore_signal(
            barrier, inc=1, device_id=(lax.rem(sp + d, N_SP), tp), device_id_type=MESH
        )
        return carry

    lax.fori_loop(1, N_SP, greet_plane, 0)

    def at_z(dz):
        return (sp, 2 * mod(z + dz, RING) + core)

    def greet_ring(d, carry):
        pl.semaphore_signal(barrier, inc=1, device_id=at_z(d), device_id_type=MESH)
        return carry

    lax.fori_loop(1, RING, greet_ring, 0)
    partner = (sp, 2 * z + (1 - core))
    pl.semaphore_signal(barrier, inc=1, device_id=partner, device_id_type=MESH)
    pl.semaphore_wait(barrier, N_SP - 1 + RING - 1 + 1)

    def remote(src, dst, send_sem, recv_sem, device):
        return pltpu.make_async_remote_copy(
            src_ref=src, dst_ref=dst, send_sem=send_sem, recv_sem=recv_sem,
            device_id=device, device_id_type=MESH,
        )

    def slot_copy(d):
        other = lax.rem(sp + d, N_SP)
        return remote(
            slots_own.at[other], rows.at[tp, sp], slot_send.at[d], slot_recv.at[d], (other, tp)
        )

    loads[0].wait()

    def send_slot(d, carry):
        slot_copy(d).start()
        return carry

    lax.fori_loop(1, N_SP, send_slot, 0)
    loads[2].wait()

    def comb_copy(d):
        return remote(comb_own, comb.at[z], comb_send.at[d], comb_recv.at[d], at_z(d))

    def send_comb(d, carry):
        comb_copy(d).start()
        return carry

    lax.fori_loop(1, RING, send_comb, 0)
    for item in loads[1:2] + loads[3:]:
        item.wait()

    def ring_copy(way, m, dz, piece):
        ref = rows.at[2 * mod(z + dz, RING) + core, pl.ds(piece * PIECE, PIECE)]
        return remote(
            ref, ref, ring_send.at[way, m], ring_recv.at[way, m], at_z(1 if way == 0 else -1)
        )

    def fwd_copy(j, dz):
        ref = rows.at[2 * mod(z + dz, RING) + core]
        return remote(ref, ref, fwd_send.at[j], fwd_recv.at[j], partner)

    def pair_copy(j):
        return remote(pair_out.at[j], pair_in.at[j], pair_send.at[j], pair_recv.at[j], partner)

    def res_copy(j, d):
        other = lax.rem(sp + d, N_SP)
        return remote(
            out.at[j, other], res.at[j, sp], res_send.at[j, d], res_recv.at[j, d], (other, tp)
        )

    def ring_event(k):
        if k == 0:
            for piece in range(2):
                def wait_slot(src, carry):
                    d = mod(sp - src, N_SP)

                    @pl.when(d != 0)
                    def _():
                        slot_copy(d).wait_recv()

                    return carry

                lax.fori_loop(piece * PIECE, (piece + 1) * PIECE, wait_slot, 0)
                for way in range(2):
                    ring_copy(way, piece, 0, piece).start()
            fwd_copy(0, 0).start()
        elif k < 4:
            for piece in range(2):
                for way in range(2):
                    dz = -k if way == 0 else k
                    ring_copy(way, 2 * (k - 1) + piece, dz, piece).wait_recv()
                    if k < 3:
                        ring_copy(way, 2 * k + piece, dz, piece).start()
                    elif piece == way:
                        ring_copy(way, 6, dz, piece).start()
            fwd_copy(2 * k - 1, -k).start()
            fwd_copy(2 * k, k).start()
        else:
            ring_copy(0, 6, 4, 0).wait_recv()
            ring_copy(1, 6, 4, 1).wait_recv()
            fwd_copy(7, 4).start()

    row_expert = lax.rem(lax.broadcasted_iota(jnp.int32, (2 * N_SP * CAP, WIDE), 0), 8) // CAP
    col_expert = lax.broadcasted_iota(jnp.int32, (2 * N_SP * CAP, WIDE), 1) // LANES
    mine = row_expert == col_expert

    def chunk_part(chunk, dst, j):
        x = rows[chunk].reshape(2 * N_SP * CAP, DEPTH)
        gate = jnp.dot(x, gate_up[:, 0:WIDE], preferred_element_type=jnp.float32)
        up = jnp.dot(x, gate_up[:, WIDE : 2 * WIDE], preferred_element_type=jnp.float32)
        inner = gate / (1.0 + jnp.exp(-gate)) * up
        inner = jnp.where(mine, inner, 0.0).astype(jnp.bfloat16)
        for n in range(DEPTH // COLS):
            cols = slice(n * COLS, (n + 1) * COLS)
            piece = jnp.dot(inner, down[:, cols], preferred_element_type=jnp.float32)
            dst[j, :, :, cols] = piece.reshape(N_SP, 8, COLS).astype(jnp.bfloat16)

    def push_results(j):
        pair_copy(j).wait_recv()
        total = own_part[j].astype(jnp.float32) + pair_in[j].astype(jnp.float32)
        out[j] = total.astype(jnp.bfloat16)
        res[j, sp] = out[j, sp]

        def push(d, carry):
            res_copy(j, d).start()
            return carry

        lax.fori_loop(1, N_SP, push, 0)

    def combine(j):
        def wait_res(d, carry):
            res_copy(j, d).wait_recv()
            return carry

        lax.fori_loop(1, N_SP, wait_res, 0)
        zj = mod(z + pick(j, Z_ORDER), RING)

        @pl.when(zj != z)
        def _():
            comb_copy(mod(z - zj, RING)).wait_recv()

        high, low = comb[zj, :, 0:LANES], comb[zj, :, LANES:WIDE]
        for n in range(DEPTH // COLS):
            cols = slice(n * COLS, (n + 1) * COLS)
            found = res[j, :, :, cols].reshape(SLOTS, COLS)
            red[j, :, cols] = jnp.dot(
                high, found, preferred_element_type=jnp.float32
            ) + jnp.dot(low, found, preferred_element_type=jnp.float32)

    def sum_copy(way, r, h):
        cols = slice(h * PART, (h + 1) * PART)
        return remote(
            sum_out.at[way, r, :, cols], sum_in.at[way, r, :, cols],
            sum_send.at[way, r, h], sum_recv.at[way, r, h], at_z(-1 if way == 0 else 1),
        )

    def far(way, h):
        return (h >= PARTS // 2) == (way == 1)

    def sum_steps(r, some):
        for h in range(PARTS // 2):
            for way in range(2):
                sum_step(way, r, h + PARTS // 2 * int((way == 1) == some))

    def sum_step(way, r, h):
        cols = slice(h * PART, (h + 1) * PART)
        d = 4 if r == 0 else (r - 4 if way == 0 else 4 - r)
        value = red[Z_PLACE[d], :, cols]
        if r > 1 or (r == 1 and far(way, h)):
            sum_copy(way, r - 1, h).wait_recv()
            value = value + sum_in[way, r - 1, :, cols].astype(jnp.float32)
        sum_out[way, r, :, cols] = value.astype(jnp.bfloat16)
        sum_copy(way, r, h).start()

    def pair_round(first, last):
        def one(j, carry):
            zj = mod(z + pick(j, Z_ORDER), RING)
            chunk_part(2 * zj + core, own_part, j)
            fwd_copy(j, 0).wait_recv()
            chunk_part(2 * zj + (1 - core), pair_out, j)
            pair_copy(j).start()

            @pl.when(j > first)
            def _():
                push_results(first)

            return carry

        lax.fori_loop(first, last + 1, one, 0)
        push_results(last)

    def combine_some(first, last):
        def one(j, carry):
            combine(j)
            return carry

        lax.fori_loop(first, last + 1, one, 0)

    def step(k, carry):
        for at in range(5):
            @pl.when(k == at)
            def _():
                ring_event(at)

        last = jnp.minimum(2 * k, RING - 1)
        pair_round(jnp.maximum(2 * k - 1, 0), last)

        @pl.when(k >= 2)
        def _():
            combine_some(jnp.maximum(2 * k - 5, 0), 2 * k - 4)

        return carry

    lax.fori_loop(0, 5, step, 0)
    combine_some(5, 6)
    sum_steps(1, False)
    combine_some(7, 7)
    sum_steps(0, True)
    sum_steps(2, False)
    sum_steps(1, True)
    sum_steps(3, False)
    sum_steps(2, True)
    sum_steps(3, True)
    for h in range(PARTS):
        cols = slice(h * PART, (h + 1) * PART)
        total = updated_ref[:, cols].astype(jnp.float32) + red[0, :, cols]
        for way in range(2):
            sum_copy(way, 3, h).wait_recv()
            total = total + sum_in[way, 3, :, cols].astype(jnp.float32)
        merged_ref[:, cols] = total.astype(jnp.bfloat16)

    def drain_plane(d, carry):
        slot_copy(d).wait_send()

        def drain_res(j, inner):
            res_copy(j, d).wait_send()
            return inner

        return lax.fori_loop(0, RING, drain_res, carry)

    lax.fori_loop(1, N_SP, drain_plane, 0)

    def drain_comb(d, carry):
        comb_copy(d).wait_send()
        return carry

    lax.fori_loop(1, RING, drain_comb, 0)

    def drain_pair(j, carry):
        fwd_copy(j, 0).wait_send()
        pair_copy(j).wait_send()
        return carry

    lax.fori_loop(0, RING, drain_pair, 0)
    for way in range(2):
        for m in range(7):
            ring_copy(way, m, 0, 0).wait_send()
        for r in range(4):
            for h in range(PARTS):
                if r > 0 or far(way, h):
                    sum_copy(way, r, h).wait_send()


def experts(slots, gate, up, down, comb, updated):
    anywhere = pl.BlockSpec(memory_space=pl.ANY)
    vmem = pl.BlockSpec(memory_space=pltpu.VMEM)
    dma = pltpu.SemaphoreType.DMA
    chunk = (N_SP, 8, DEPTH)
    bf16, f32 = jnp.bfloat16, jnp.float32
    return pl.pallas_call(
        expert_kernel,
        out_shape=jax.ShapeDtypeStruct((ROWS, DEPTH), bf16),
        in_specs=[anywhere] * 5 + [vmem],
        out_specs=vmem,
        scratch_shapes=[
            pltpu.VMEM(chunk, bf16),
            pltpu.VMEM((N_TP, *chunk), bf16),
            pltpu.VMEM((DEPTH, 2 * WIDE), bf16),
            pltpu.VMEM((WIDE, DEPTH), bf16),
            pltpu.VMEM((ROWS, WIDE), bf16),
            pltpu.VMEM((RING, ROWS, WIDE), bf16),
            pltpu.VMEM((RING, *chunk), bf16),
            pltpu.VMEM((RING, *chunk), bf16),
            pltpu.VMEM((RING, *chunk), bf16),
            pltpu.VMEM((RING, *chunk), bf16),
            pltpu.VMEM((RING, *chunk), bf16),
            pltpu.VMEM((RING, ROWS, DEPTH), f32),
            pltpu.VMEM((2, 4, ROWS, DEPTH), bf16),
            pltpu.VMEM((2, 4, ROWS, DEPTH), bf16),
            dma((10,)),
            dma((N_SP,)),
            dma((N_SP,)),
            dma((2, 7)),
            dma((2, 7)),
            dma((RING,)),
            dma((RING,)),
            dma((RING,)),
            dma((RING,)),
            dma((RING, N_SP)),
            dma((RING, N_SP)),
            dma((RING,)),
            dma((RING,)),
            dma((2, 4, PARTS)),
            dma((2, 4, PARTS)),
        ],
        compiler_params=pltpu.CompilerParams(
            collective_id=1, has_side_effects=True, vmem_limit_bytes=56 * 1024 * 1024
        ),
        name="experts",
    )(slots, gate, up, down, comb, updated)


def shards(
    queries, key_pairs, head_values, lambdas, head_gain, out_weight, residual, norm_gain,
    expert_ids, route_weights, gate_weight, up_weight, down_weight,
):
    q = queries.reshape(N_SP, ROWS, LANES)
    across = head_values.reshape(SPAN // LANES, LANES, LANES).swapaxes(1, 2)
    kv = jnp.stack(
        [key_pairs.reshape(2, HALF, LANES), across.reshape(2, HALF, LANES)], axis=1
    )
    flat_ids = expert_ids.reshape(-1)
    routes = flat_ids.shape[0]
    same = flat_ids[:, None] == flat_ids[None, :]
    earlier = jnp.arange(routes)[:, None] > jnp.arange(routes)[None, :]
    ranking = jnp.sum((same & earlier).astype(jnp.int32), axis=1)
    slots = (flat_ids * CAP + ranking).reshape(ROWS, 2)
    hit = slots[:, :, None] == jnp.arange(SLOTS, dtype=jnp.int32)[None, None, :]
    select = jnp.any(hit, axis=1).T.astype(jnp.bfloat16)
    weight = jnp.sum(jnp.where(hit, route_weights[:, :, None], 0.0), axis=1)
    high = weight.astype(jnp.bfloat16)
    low = (weight - high.astype(jnp.float32)).astype(jnp.bfloat16)
    updated, outgoing = attend(
        q, kv, out_weight, lambdas.reshape(1, 1), head_gain.reshape(1, LANES), select,
        residual, norm_gain.reshape(1, DEPTH),
    )
    return experts(
        outgoing, gate_weight, up_weight, down_weight, jnp.concatenate([high, low], axis=1),
        updated,
    )


def solution(mesh):
    in_specs = (
        P("sp", "tp", None),
        P("sp", "tp", None),
        P("sp", "tp", None),
        P("tp"),
        P(),
        P(),
        P(("sp", "tp"), None),
        P(),
        P(("sp", "tp"), None),
        P(("sp", "tp"), None),
        P("sp", None, "tp"),
        P("sp", None, "tp"),
        P("sp", "tp", None),
    )
    return jax.shard_map(
        shards, mesh=mesh, in_specs=in_specs, out_specs=P(("sp", "tp"), None), check_vma=False
    )
```

```python
import jax
import jax.numpy as jnp
from jax import lax
from jax.experimental import pallas as pl
from jax.experimental.pallas import tpu as pltpu
from jax.sharding import PartitionSpec as P

MESH = pl.DeviceIdType.MESH
SIDE = 4
N_SP = 16
N_TP = 16
ROWS = 48
SPAN = N_TP * ROWS
HALF = SPAN // 2
LANES = 128
TILES = SPAN // LANES
ONES = 16
HD = 64
DEPTH = 2048
EXPERTS = 32
CAP = 4
SLOTS = EXPERTS * CAP
COLS = 512
NEG = -1e30

ORDER = [
    (0, 0), (-1, 0), (1, 0), (0, -1), (0, 1), (2, 0), (-1, -1), (-1, 1),
    (1, -1), (1, 1), (2, -1), (2, 1), (0, 2), (-1, 2), (1, 2), (2, 2),
]
PLACE = {0: 0, -1: 1, 1: 2, 2: 3}


def pick(index, values):
    out = jnp.int32(values[0])
    for k, value in enumerate(values):
        out = jnp.where(index == k, jnp.int32(value), out)
    return out


def mod(value, size):
    return lax.rem(value + size, size)


def attend_part(
    lam_ref, gain_ref, select_ref, residual_ref, norm_gain_ref,
    load_q, load_kv, load_w, send_comb, owner, keeps,
    updated_ref, slots_ref,
    q_own, q_land, qs, kvb, acc, top, score_a, score_b, weight_a, weight_b,
    own_heads, heads, w_vmem,
    q_send, q_recv, kv_send, kv_recv, head_send, head_recv,
):
    sp = lax.axis_index("sp")
    tp = lax.axis_index("tp")
    x, y = lax.rem(sp, SIDE), sp // SIDE

    load_q.wait()

    def row_block(g):
        return pl.ds(pl.multiple_of(g * ROWS, ROWS), ROWS)

    def q_copy(d):
        other = lax.rem(sp + d, N_SP)
        return pltpu.make_async_remote_copy(
            src_ref=q_own.at[owner(other, sp)], dst_ref=q_land.at[row_block(sp)],
            send_sem=q_send.at[d], recv_sem=q_recv.at[d],
            device_id=(other, tp), device_id_type=MESH,
        )

    def send_q(d, carry):
        q_copy(d).start()
        return carry

    lax.fori_loop(1, N_SP, send_q, 0)
    load_kv.wait()

    def block_of(half, du, dv):
        dx, dy = (du, dv) if half == 0 else (dv, du)
        return mod(y + dy, SIDE) * SIDE + mod(x + dx, SIDE)

    def kv_copy(half, index, block, part, du, dv):
        ref = kvb.at[block, half] if part is None else kvb.at[block, half, part]
        return pltpu.make_async_remote_copy(
            src_ref=ref, dst_ref=ref,
            send_sem=kv_send.at[half, index], recv_sem=kv_recv.at[half, index],
            device_id=(block_of(half, du, dv), tp), device_id_type=MESH,
        )

    def send(half, index, rel, part, du, dv):
        kv_copy(half, index, block_of(half, *rel), part, du, dv).start()

    def arrived(half, index, rel, part):
        kv_copy(half, index, block_of(half, *rel), part, 1, 0).wait_recv()

    for half in range(2):
        send(half, 0, (0, 0), None, 1, 0)
        send(half, 1, (0, 0), None, -1, 0)
        send(half, 4, (0, 0), None, 0, 1)
        send(half, 8, (0, 0), None, 0, -1)
    send_comb()

    for own in range(N_SP):
        @pl.when(sp == own)
        def _():
            q_land[own * ROWS : (own + 1) * ROWS] = q_own[2 * own % N_TP]

    def wait_q(d, carry):
        q_copy(d).wait_recv()
        return carry

    lax.fori_loop(1, N_SP, wait_q, 0)

    lane = lax.broadcasted_iota(jnp.int32, (LANES, LANES), 1)
    for i in range(TILES):
        wide = q_land[i * LANES : (i + 1) * LANES].astype(jnp.float32) * (HD**-0.5)
        qs[i, 0:LANES] = jnp.where(lane < HD, wide, 0.0).astype(jnp.bfloat16)
        qs[i, LANES : 2 * LANES] = jnp.where(lane >= HD, wide, 0.0).astype(jnp.bfloat16)
    acc[...] = jnp.zeros_like(acc)
    top[...] = jnp.full_like(top, NEG)

    score_bufs, weight_bufs = (score_a, score_b), (weight_a, weight_b)

    def tiles_step(first, block, half):
        keys = kvb[block, half, 0]
        wide = jnp.concatenate(
            [kvb[block, half, 1, k * LANES : (k + 1) * LANES] for k in range(HALF // LANES)],
            axis=1,
        )
        wide = jnp.concatenate([wide, jnp.ones((ONES, HALF), jnp.bfloat16)], axis=0)

        def score(i):
            scores = lax.dot_general(
                keys, qs[i], (((1,), (1,)), ((), ())), preferred_element_type=jnp.float32
            )
            if i < first + 3:
                place = lax.broadcasted_iota(jnp.int32, (1, LANES), 1) + i * LANES
                span = lax.shift_right_logical(place * 1366, 16)
                last = (
                    span * (SPAN - ROWS) + place + ((sp + span) & (N_TP - 1)) * ROWS
                    - block * SPAN - half * HALF
                )
                kept = lax.broadcasted_iota(jnp.int32, (HALF, LANES), 0) <= last
                scores = jnp.where(jnp.concatenate([kept, kept], axis=1), scores, -jnp.inf)
            score_bufs[i % 2][...] = scores
            old_top = top[i]
            new_top = jnp.maximum(old_top, jnp.max(scores, axis=0, keepdims=True))
            top[i] = new_top
            return new_top, jnp.exp(old_top - new_top)

        def weigh(i, new_top):
            weights = jnp.exp(score_bufs[i % 2][...] - new_top)
            weight_bufs[i % 2][...] = weights.astype(jnp.bfloat16)

        def add_up(i, decay):
            fresh = jnp.dot(wide, weight_bufs[i % 2][...], preferred_element_type=jnp.float32)
            acc[i] = acc[i] * decay + fresh

        state = {first: score(first)}
        for i in range(first, TILES + 1):
            if i + 1 < TILES:
                state[i + 1] = score(i + 1)
            if i < TILES:
                weigh(i, state[i][0])
            if i > first:
                add_up(i - 1, state[i - 1][1])

    def use_block(block, half):
        first = block * ROWS // LANES // 2
        for k in range(TILES // 2):
            @pl.when(first == k)
            def _():
                tiles_step(2 * k, block, half)

    def step(s, carry):
        def on(k, half):
            du, dv = ORDER[k]
            if k == 1:
                arrived(half, 0, (-1, 0), None)
                send(half, 2, (-1, 0), 0, 1, 0)
                send(half, 5, (-1, 0), None, 0, 1)
                send(half, 9, (-1, 0), None, 0, -1)
            elif k == 2:
                arrived(half, 1, (1, 0), None)
                send(half, 3, (1, 0), 1, -1, 0)
                send(half, 6, (1, 0), None, 0, 1)
                send(half, 10, (1, 0), None, 0, -1)
            elif k == 5:
                arrived(half, 2, (2, 0), 0)
                arrived(half, 3, (2, 0), 1)
                send(half, 7, (2, 0), None, 0, 1)
                send(half, 11, (2, 0), None, 0, -1)
            elif dv == -1:
                place = PLACE[du]
                arrived(half, 4 + place, (du, dv), None)
                send(half, 12 + place, (du, dv), 0, 0, 1)
            elif dv == 1:
                place = PLACE[du]
                arrived(half, 8 + place, (du, dv), None)
                send(half, 16 + place, (du, dv), 1, 0, -1)
            elif dv == 2:
                place = PLACE[du]
                arrived(half, 12 + place, (du, dv), 0)
                arrived(half, 16 + place, (du, dv), 1)

        for k in range(1, len(ORDER)):
            @pl.when(s == k)
            def _():
                for half in range(2):
                    on(k, half)

        du = pick(s, [o[0] for o in ORDER])
        dv = pick(s, [o[1] for o in ORDER])

        def one_half(half, carry):
            dx = jnp.where(half == 0, du, dv)
            dy = jnp.where(half == 0, dv, du)
            block = mod(y + dy, SIDE) * SIDE + mod(x + dx, SIDE)
            use_block(block, half)
            return carry

        return lax.fori_loop(0, 2, one_half, carry)

    lax.fori_loop(0, len(ORDER), step, 0)

    lam = lam_ref[0, 0]

    for i in range(TILES):
        ratio = acc[i, 0:LANES] / acc[i, LANES : LANES + 1]
        mixed = ratio[:, 0:LANES] - lam * ratio[:, LANES : 2 * LANES]
        square = jnp.mean(mixed * mixed, axis=0, keepdims=True)
        done = (mixed * lax.rsqrt(square + 1e-06)).T * gain_ref[...]
        own_heads[i * LANES : (i + 1) * LANES] = done.astype(jnp.bfloat16)

    def head_copy(g, h):
        return pltpu.make_async_remote_copy(
            src_ref=own_heads.at[row_block(g)],
            dst_ref=heads.at[:, pl.ds(pl.multiple_of(tp * LANES, LANES), LANES)],
            send_sem=head_send.at[g], recv_sem=head_recv.at[h],
            device_id=(g, owner(sp, g)), device_id_type=MESH,
        )

    def push_head(g, carry):
        @pl.when(jnp.logical_or(g != sp, jnp.logical_not(keeps)))
        def _():
            head_copy(g, tp).start()

        return carry

    lax.fori_loop(0, N_SP, push_head, 0)

    for own in range(N_SP):
        @pl.when(jnp.logical_and(sp == own, keeps))
        def _():
            at = 2 * own % N_TP * LANES
            heads[:, at : at + LANES] = own_heads[own * ROWS : (own + 1) * ROWS]

    load_w.wait()

    def wait_head(h, carry):
        @pl.when(jnp.logical_or(h != tp, jnp.logical_not(keeps)))
        def _():
            head_copy(0, h).wait_recv()

        return carry

    lax.fori_loop(0, N_TP, wait_head, 0)

    attended = heads[...]
    squares = jnp.zeros((ROWS, 1), jnp.float32)
    wide = []
    for n in range(DEPTH // COLS):
        cols = slice(n * COLS, (n + 1) * COLS)
        projected = jnp.dot(attended, w_vmem[:, cols], preferred_element_type=jnp.float32)
        updated = (residual_ref[:, cols].astype(jnp.float32) + projected).astype(jnp.bfloat16)
        updated_ref[:, cols] = updated
        back = updated.astype(jnp.float32)
        squares = squares + jnp.sum(back * back, axis=1, keepdims=True)
        wide.append(back)
    scale = lax.rsqrt(squares / DEPTH + 1e-06)
    for n in range(DEPTH // COLS):
        cols = slice(n * COLS, (n + 1) * COLS)
        normed = (wide[n] * scale * norm_gain_ref[:, cols]).astype(jnp.bfloat16)
        packed = jnp.dot(select_ref[...], normed, preferred_element_type=jnp.float32)
        slots_ref[:, :, cols] = packed.reshape(N_SP, 8, COLS).astype(jnp.bfloat16)

    def drain():
        def drain_q(d, carry):
            q_copy(d).wait_send()
            return carry

        lax.fori_loop(1, N_SP, drain_q, 0)

        def drain_heads(g, carry):
            @pl.when(jnp.logical_or(g != sp, jnp.logical_not(keeps)))
            def _():
                head_copy(g, tp).wait_send()

            return carry

        lax.fori_loop(0, N_SP, drain_heads, 0)
        for half in range(2):
            for index in range(20):
                part = None if index in (0, 1) or 4 <= index < 12 else 0
                kv_copy(half, index, sp, part, 1, 0).wait_send()

    return drain


RING = 8
PIECE = 8
WIDE = 2 * LANES
EARLY = 1536
LATE = DEPTH - EARLY
PARTS = 4
PART = EARLY // PARTS
LATE_PART = LATE // 2
Z_ORDER = [0, -1, 1, -2, 2, -3, 3, 4]
SPREAD = [0, 1, 3, 4, 12, 5, 7, 8, 13, 15, 2, 6, 9, 11, 14, 10]
Z_PLACE = {d: k for k, d in enumerate(Z_ORDER)}


def expert_part(
    slots_own, updated_ref, loads, comb_copy,
    merged_ref,
    rows, gate_up, down, comb, own_part, pair_out, pair_in, out,
    res, red, sum_out, sum_in, tail_out, tail_in, whole_out, whole_in,
    slot_send, slot_recv, ring_send, ring_recv, fwd_send, fwd_recv,
    pair_send, pair_recv, res_send, res_recv, sum_send, sum_recv,
    tail_send, tail_recv, whole_send, whole_recv,
):
    sp = lax.axis_index("sp")
    tp = lax.axis_index("tp")
    z, core = tp // 2, lax.rem(tp, 2)
    x, y = lax.rem(sp, SIDE), sp // SIDE

    def at_z(dz):
        return (sp, 2 * mod(z + dz, RING) + core)

    partner = (sp, 2 * z + (1 - core))

    def remote(src, dst, send_sem, recv_sem, device):
        return pltpu.make_async_remote_copy(
            src_ref=src, dst_ref=dst, send_sem=send_sem, recv_sem=recv_sem,
            device_id=device, device_id_type=MESH,
        )

    def peer(d):
        return mod(y + d // SIDE, SIDE) * SIDE + mod(x + lax.rem(d, SIDE), SIDE)

    def slot_copy(d):
        other = peer(d)
        return remote(
            slots_own.at[other], rows.at[tp, sp], slot_send.at[d], slot_recv.at[d], (other, tp)
        )

    def send_slot(n, carry):
        slot_copy(pick(n, SPREAD)).start()
        return carry

    lax.fori_loop(1, N_SP, send_slot, 0)
    rows[tp, sp] = slots_own[sp]
    for item in loads:
        item.wait()

    def ring_copy(way, m, dz, piece):
        ref = rows.at[2 * mod(z + dz, RING) + core, pl.ds(piece * PIECE, PIECE)]
        return remote(
            ref, ref, ring_send.at[way, m], ring_recv.at[way, m], at_z(1 if way == 0 else -1)
        )

    def fwd_copy(j, dz):
        ref = rows.at[2 * mod(z + dz, RING) + core]
        return remote(ref, ref, fwd_send.at[j], fwd_recv.at[j], partner)

    def pair_copy(j):
        return remote(pair_out.at[j], pair_in.at[j], pair_send.at[j], pair_recv.at[j], partner)

    def res_copy(j, d):
        other = peer(d)
        return remote(
            out.at[j, other, :, 0:EARLY], res.at[j, sp, :, 0:EARLY],
            res_send.at[j, d], res_recv.at[j, d], (other, tp),
        )

    def ring_event(k):
        if k == 0:
            for piece in range(2):
                def wait_slot(src, carry):
                    d = mod(y - src // SIDE, SIDE) * SIDE + mod(x - lax.rem(src, SIDE), SIDE)

                    @pl.when(d != 0)
                    def _():
                        slot_copy(d).wait_recv()

                    return carry

                lax.fori_loop(piece * PIECE, (piece + 1) * PIECE, wait_slot, 0)
                for way in range(2):
                    ring_copy(way, piece, 0, piece).start()
            fwd_copy(0, 0).start()
        elif k < 4:
            for piece in range(2):
                for way in range(2):
                    dz = -k if way == 0 else k
                    ring_copy(way, 2 * (k - 1) + piece, dz, piece).wait_recv()
                    if k < 3:
                        ring_copy(way, 2 * k + piece, dz, piece).start()
                    elif piece == way:
                        ring_copy(way, 6, dz, piece).start()
            fwd_copy(2 * k - 1, -k).start()
            fwd_copy(2 * k, k).start()
        else:
            ring_copy(0, 6, 4, 0).wait_recv()
            ring_copy(1, 6, 4, 1).wait_recv()
            fwd_copy(7, 4).start()

    row_expert = lax.rem(lax.broadcasted_iota(jnp.int32, (2 * N_SP * CAP, WIDE), 0), 8) // CAP
    col_expert = lax.broadcasted_iota(jnp.int32, (2 * N_SP * CAP, WIDE), 1) // LANES
    mine = row_expert == col_expert

    def chunk_part(chunk, dst, j):
        x = rows[chunk].reshape(2 * N_SP * CAP, DEPTH)
        gate = jnp.dot(x, gate_up[:, 0:WIDE], preferred_element_type=jnp.float32)
        up = jnp.dot(x, gate_up[:, WIDE : 2 * WIDE], preferred_element_type=jnp.float32)
        inner = gate / (1.0 + jnp.exp(-gate)) * up
        inner = jnp.where(mine, inner, 0.0).astype(jnp.bfloat16)
        for n in range(DEPTH // COLS):
            cols = slice(n * COLS, (n + 1) * COLS)
            piece = jnp.dot(inner, down[:, cols], preferred_element_type=jnp.float32)
            dst[j, :, :, cols] = piece.reshape(N_SP, 8, COLS).astype(jnp.bfloat16)

    def push_results(j):
        pair_copy(j).wait_recv()
        total = own_part[j].astype(jnp.float32) + pair_in[j].astype(jnp.float32)
        out[j] = total.astype(jnp.bfloat16)
        res[j, sp, :, 0:EARLY] = out[j, sp, :, 0:EARLY]

        def push(n, carry):
            res_copy(j, pick(n, SPREAD)).start()
            return carry

        lax.fori_loop(1, N_SP, push, 0)

    def combine(j):
        def wait_res(d, carry):
            res_copy(j, d).wait_recv()
            return carry

        lax.fori_loop(1, N_SP, wait_res, 0)
        zj = mod(z + pick(j, Z_ORDER), RING)

        @pl.when(zj != z)
        def _():
            comb_copy(mod(z - zj, RING)).wait_recv()

        high, low = comb[zj, :, 0:LANES], comb[zj, :, LANES:WIDE]
        for n in range(EARLY // COLS):
            cols = slice(n * COLS, (n + 1) * COLS)
            found = res[j, :, :, cols].reshape(SLOTS, COLS)
            red[j, :, cols] = jnp.dot(
                high, found, preferred_element_type=jnp.float32
            ) + jnp.dot(low, found, preferred_element_type=jnp.float32)

    def tail_copy(way, r, h):
        cols = slice(h * LATE_PART, (h + 1) * LATE_PART)
        return remote(
            tail_out.at[way, r, :, :, cols], tail_in.at[way, r, :, :, cols],
            tail_send.at[way, r, h], tail_recv.at[way, r, h], at_z(-1 if way == 0 else 1),
        )

    def tail_step(way, r, h):
        cols = slice(h * LATE_PART, (h + 1) * LATE_PART)
        d = 4 if r == 0 else (r - 4 if way == 0 else 4 - r)
        value = out[Z_PLACE[d], :, :, EARLY + h * LATE_PART : EARLY + (h + 1) * LATE_PART]
        if r > 1 or (r == 1 and h == way):
            tail_copy(way, r - 1, h).wait_recv()
            there = tail_in[way, r - 1, :, :, cols].astype(jnp.float32)
            value = (value.astype(jnp.float32) + there).astype(jnp.bfloat16)
        tail_out[way, r, :, :, cols] = value
        tail_copy(way, r, h).start()

    def tail_steps(r, some):
        for way in range(2):
            tail_step(way, r, way if some else 1 - way)

    def whole_copy(d):
        other = peer(d)
        return remote(
            whole_out.at[other], whole_in.at[sp], whole_send.at[d], whole_recv.at[d], (other, tp)
        )

    def push_whole():
        for h in range(2):
            cols = slice(h * LATE_PART, (h + 1) * LATE_PART)
            at = slice(EARLY + h * LATE_PART, EARLY + (h + 1) * LATE_PART)
            total = out[0, :, :, at].astype(jnp.float32)
            for way in range(2):
                tail_copy(way, 3, h).wait_recv()
                total = total + tail_in[way, 3, :, :, cols].astype(jnp.float32)
            whole_out[:, :, cols] = total.astype(jnp.bfloat16)
        whole_in[sp] = whole_out[sp]

        def push(n, carry):
            whole_copy(pick(n, SPREAD)).start()
            return carry

        lax.fori_loop(1, N_SP, push, 0)

    def sum_copy(way, r, h):
        cols = slice(h * PART, (h + 1) * PART)
        return remote(
            sum_out.at[way, r, :, cols], sum_in.at[way, r, :, cols],
            sum_send.at[way, r, h], sum_recv.at[way, r, h], at_z(-1 if way == 0 else 1),
        )

    def far(way, h):
        return (h >= PARTS // 2) == (way == 1)

    def sum_steps(r, some):
        for h in range(PARTS // 2):
            for way in range(2):
                sum_step(way, r, h + PARTS // 2 * int((way == 1) == some))

    def sum_step(way, r, h):
        cols = slice(h * PART, (h + 1) * PART)
        d = 4 if r == 0 else (r - 4 if way == 0 else 4 - r)
        value = red[Z_PLACE[d], :, cols]
        if r > 1 or (r == 1 and far(way, h)):
            sum_copy(way, r - 1, h).wait_recv()
            value = value + sum_in[way, r - 1, :, cols].astype(jnp.float32)
        sum_out[way, r, :, cols] = value.astype(jnp.bfloat16)
        sum_copy(way, r, h).start()

    def pair_round(first, last):
        def one(j, carry):
            zj = mod(z + pick(j, Z_ORDER), RING)
            chunk_part(2 * zj + core, own_part, j)
            fwd_copy(j, 0).wait_recv()
            chunk_part(2 * zj + (1 - core), pair_out, j)
            pair_copy(j).start()

            @pl.when(j > first)
            def _():
                push_results(first)

            return carry

        lax.fori_loop(first, last + 1, one, 0)
        push_results(last)

    def combine_some(first, last):
        def one(j, carry):
            combine(j)
            return carry

        lax.fori_loop(first, last + 1, one, 0)

    def step(k, carry):
        for at in range(5):
            @pl.when(k == at)
            def _():
                ring_event(at)

        last = jnp.minimum(2 * k, RING - 1)
        pair_round(jnp.maximum(2 * k - 1, 0), last)

        @pl.when(jnp.logical_or(k == 2, k == 3))
        def _():
            combine_some(jnp.maximum(2 * k - 5, 0), 2 * k - 4)

        return carry

    lax.fori_loop(0, 5, step, 0)
    tail_steps(1, False)
    tail_steps(0, True)
    combine_some(3, 4)
    tail_steps(2, False)
    tail_steps(1, True)
    combine_some(5, 5)
    tail_steps(3, False)
    tail_steps(2, True)
    combine_some(6, 6)
    tail_steps(3, True)
    sum_steps(1, False)
    combine_some(7, 7)
    sum_steps(0, True)
    push_whole()
    sum_steps(2, False)
    sum_steps(1, True)
    sum_steps(3, False)
    sum_steps(2, True)
    sum_steps(3, True)

    def wait_whole(d, carry):
        whole_copy(d).wait_recv()
        return carry

    lax.fori_loop(1, N_SP, wait_whole, 0)
    found = whole_in[...].reshape(SLOTS, LATE)
    total = updated_ref[:, EARLY:DEPTH].astype(jnp.float32)
    for part in (comb[z, :, 0:LANES], comb[z, :, LANES:WIDE]):
        total = total + jnp.dot(part, found, preferred_element_type=jnp.float32)
    merged_ref[:, EARLY:DEPTH] = total.astype(jnp.bfloat16)
    for h in range(PARTS):
        cols = slice(h * PART, (h + 1) * PART)
        total = updated_ref[:, cols].astype(jnp.float32) + red[0, :, cols]
        for way in range(2):
            sum_copy(way, 3, h).wait_recv()
            total = total + sum_in[way, 3, :, cols].astype(jnp.float32)
        merged_ref[:, cols] = total.astype(jnp.bfloat16)

    def drain_plane(d, carry):
        slot_copy(d).wait_send()
        whole_copy(d).wait_send()

        def drain_res(j, inner):
            res_copy(j, d).wait_send()
            return inner

        return lax.fori_loop(0, RING, drain_res, carry)

    lax.fori_loop(1, N_SP, drain_plane, 0)

    def drain_pair(j, carry):
        fwd_copy(j, 0).wait_send()
        pair_copy(j).wait_send()
        return carry

    lax.fori_loop(0, RING, drain_pair, 0)
    for way in range(2):
        for m in range(7):
            ring_copy(way, m, 0, 0).wait_send()
        for r in range(4):
            for h in range(2):
                if r > 0 or h == way:
                    tail_copy(way, r, h).wait_send()
            for h in range(PARTS):
                if r > 0 or far(way, h):
                    sum_copy(way, r, h).wait_send()


def layer_kernel(
    q_hbm, kv_hbm, w_hbm, gate_hbm, up_hbm, down_hbm, comb_hbm,
    lam_ref, gain_ref, select_ref, residual_ref, norm_gain_ref,
    merged_ref,
    *scratch,
):
    (q_own, q_land, qs, kvb, acc, top, score_a, score_b, weight_a, weight_b,
     own_heads, heads, w_vmem, updated_ref, slots_own,
     rows, gate_up, down, comb_own, comb, own_part, pair_out, pair_in, out,
     res, red, sum_out, sum_in, tail_out, tail_in, whole_out, whole_in,
     local_sem, q_send, q_recv, kv_send, kv_recv, head_send, head_recv,
     slot_send, slot_recv, ring_send, ring_recv, fwd_send, fwd_recv,
     pair_send, pair_recv, res_send, res_recv, comb_send, comb_recv, sum_send, sum_recv,
     tail_send, tail_recv, whole_send, whole_recv) = scratch
    sp = lax.axis_index("sp")
    tp = lax.axis_index("tp")
    z, core = tp // 2, lax.rem(tp, 2)

    barrier = pltpu.get_barrier_semaphore()

    def load(k, src, dst):
        return pltpu.make_async_copy(src, dst, local_sem.at[k])

    load_q = load(0, q_hbm, q_own)
    load_kv = load(1, kv_hbm, kvb.at[sp])
    load_comb = [load(2, comb_hbm, comb_own), load(3, comb_hbm, comb.at[z])]
    load_w = load(4, w_hbm, w_vmem)
    loads = []
    for e in range(2):
        loads += [
            load(5 + e, gate_hbm.at[e], gate_up.at[:, e * LANES : (e + 1) * LANES]),
            load(7 + e, up_hbm.at[e], gate_up.at[:, (2 + e) * LANES : (3 + e) * LANES]),
            load(9 + e, down_hbm.at[e], down.at[e * LANES : (e + 1) * LANES]),
        ]
    for item in [load_q, load_kv, *load_comb, load_w, *loads]:
        item.start()

    def greet(*device):
        pl.semaphore_signal(barrier, inc=1, device_id=device, device_id_type=MESH)

    def greet_plane(d, carry):
        greet(lax.rem(sp + d, N_SP), tp)
        return carry

    lax.fori_loop(1, N_SP, greet_plane, 0)

    def owner(i, b):
        return lax.rem(i + b, N_TP)

    source = mod(tp - sp, N_SP)
    keeps = owner(sp, sp) == tp

    def greet_sources(h, carry):
        @pl.when(jnp.logical_or(jnp.logical_not(keeps), h != tp))
        def _():
            greet(source, h)

        return carry

    lax.fori_loop(0, N_TP, greet_sources, 0)

    def plane_z(d):
        return 2 * lax.rem(z + d, RING) + core

    def greet_ring(d, carry):
        greet(sp, plane_z(d))
        return carry

    lax.fori_loop(1, RING, greet_ring, 0)
    greet(sp, 2 * z + (1 - core))
    pl.semaphore_wait(
        barrier,
        N_SP - 1 + N_TP + RING - jnp.where(keeps, jnp.int32(1), jnp.int32(0)),
    )

    def comb_copy(d):
        return pltpu.make_async_remote_copy(
            src_ref=comb_own, dst_ref=comb.at[z],
            send_sem=comb_send.at[d], recv_sem=comb_recv.at[d],
            device_id=(sp, plane_z(d)), device_id_type=MESH,
        )

    def send_comb():
        for item in load_comb:
            item.wait()

        def one(d, carry):
            comb_copy(d).start()
            return carry

        lax.fori_loop(1, RING, one, 0)

    drain_attend = attend_part(
        lam_ref, gain_ref, select_ref, residual_ref, norm_gain_ref,
        load_q, load_kv, load_w, send_comb, owner, keeps,
        updated_ref, slots_own,
        q_own, q_land, qs, kvb, acc, top, score_a, score_b, weight_a, weight_b,
        own_heads, heads, w_vmem,
        q_send, q_recv, kv_send, kv_recv, head_send, head_recv,
    )
    expert_part(
        slots_own, updated_ref, loads, comb_copy,
        merged_ref,
        rows, gate_up, down, comb, own_part, pair_out, pair_in, out,
        res, red, sum_out, sum_in, tail_out, tail_in, whole_out, whole_in,
        slot_send, slot_recv, ring_send, ring_recv, fwd_send, fwd_recv,
        pair_send, pair_recv, res_send, res_recv, sum_send, sum_recv,
        tail_send, tail_recv, whole_send, whole_recv,
    )
    drain_attend()

    def drain_comb(d, carry):
        comb_copy(d).wait_send()
        return carry

    lax.fori_loop(1, RING, drain_comb, 0)


def layer(q, kv, w, gate, up, down, comb, lam, gain, select, residual, norm_gain):
    anywhere = pl.BlockSpec(memory_space=pl.ANY)
    vmem = pl.BlockSpec(memory_space=pltpu.VMEM)
    smem = pl.BlockSpec(memory_space=pltpu.SMEM)
    dma = pltpu.SemaphoreType.DMA
    chunk = (N_SP, 8, DEPTH)
    bf16, f32 = jnp.bfloat16, jnp.float32
    return pl.pallas_call(
        layer_kernel,
        out_shape=jax.ShapeDtypeStruct((ROWS, DEPTH), bf16),
        in_specs=[anywhere] * 7 + [smem, vmem, vmem, vmem, vmem],
        out_specs=vmem,
        scratch_shapes=[
            pltpu.VMEM((N_SP, ROWS, LANES), bf16),
            pltpu.VMEM((SPAN, LANES), bf16),
            pltpu.VMEM((TILES, 2 * LANES, LANES), bf16),
            pltpu.VMEM((N_SP, 2, 2, HALF, LANES), bf16),
            pltpu.VMEM((TILES, LANES + ONES, 2 * LANES), f32),
            pltpu.VMEM((TILES, 1, 2 * LANES), f32),
            pltpu.VMEM((HALF, 2 * LANES), f32),
            pltpu.VMEM((HALF, 2 * LANES), f32),
            pltpu.VMEM((HALF, 2 * LANES), bf16),
            pltpu.VMEM((HALF, 2 * LANES), bf16),
            pltpu.VMEM((SPAN, LANES), bf16),
            pltpu.VMEM((ROWS, DEPTH), bf16),
            pltpu.VMEM((DEPTH, DEPTH), bf16),
            pltpu.VMEM((ROWS, DEPTH), bf16),
            pltpu.VMEM(chunk, bf16),
            pltpu.VMEM((N_TP, *chunk), bf16),
            pltpu.VMEM((DEPTH, 2 * WIDE), bf16),
            pltpu.VMEM((WIDE, DEPTH), bf16),
            pltpu.VMEM((ROWS, WIDE), bf16),
            pltpu.VMEM((RING, ROWS, WIDE), bf16),
            pltpu.VMEM((RING, *chunk), bf16),
            pltpu.VMEM((RING, *chunk), bf16),
            pltpu.VMEM((RING, *chunk), bf16),
            pltpu.VMEM((RING, *chunk), bf16),
            pltpu.VMEM((RING, *chunk), bf16),
            pltpu.VMEM((RING, ROWS, EARLY), f32),
            pltpu.VMEM((2, 4, ROWS, EARLY), bf16),
            pltpu.VMEM((2, 4, ROWS, EARLY), bf16),
            pltpu.VMEM((2, 4, N_SP, 8, LATE), bf16),
            pltpu.VMEM((2, 4, N_SP, 8, LATE), bf16),
            pltpu.VMEM((N_SP, 8, LATE), bf16),
            pltpu.VMEM((N_SP, 8, LATE), bf16),
            dma((11,)),
            dma((N_SP,)),
            dma((N_SP,)),
            dma((2, 20)),
            dma((2, 20)),
            dma((N_SP,)),
            dma((N_TP,)),
            dma((N_SP,)),
            dma((N_SP,)),
            dma((2, 7)),
            dma((2, 7)),
            dma((RING,)),
            dma((RING,)),
            dma((RING,)),
            dma((RING,)),
            dma((RING, N_SP)),
            dma((RING, N_SP)),
            dma((RING,)),
            dma((RING,)),
            dma((2, 4, PARTS)),
            dma((2, 4, PARTS)),
            dma((2, 4, 2)),
            dma((2, 4, 2)),
            dma((N_SP,)),
            dma((N_SP,)),
        ],
        compiler_params=pltpu.CompilerParams(
            collective_id=0, has_side_effects=True, vmem_limit_bytes=63 * 1024 * 1024
        ),
        name="layer",
    )(q, kv, w, gate, up, down, comb, lam, gain, select, residual, norm_gain)


def shards(
    queries, key_pairs, head_values, lambdas, head_gain, out_weight, residual, norm_gain,
    expert_ids, route_weights, gate_weight, up_weight, down_weight,
):
    q = queries.reshape(N_SP, ROWS, LANES)
    across = head_values.reshape(SPAN // LANES, LANES, LANES).swapaxes(1, 2)
    kv = jnp.stack(
        [key_pairs.reshape(2, HALF, LANES), across.reshape(2, HALF, LANES)], axis=1
    )
    flat_ids = expert_ids.reshape(-1)
    routes = flat_ids.shape[0]
    same = flat_ids[:, None] == flat_ids[None, :]
    earlier = jnp.arange(routes)[:, None] > jnp.arange(routes)[None, :]
    ranking = jnp.sum((same & earlier).astype(jnp.int32), axis=1)
    slots = (flat_ids * CAP + ranking).reshape(ROWS, 2)
    hit = slots[:, :, None] == jnp.arange(SLOTS, dtype=jnp.int32)[None, None, :]
    select = jnp.any(hit, axis=1).T.astype(jnp.bfloat16)
    weight = jnp.sum(jnp.where(hit, route_weights[:, :, None], 0.0), axis=1)
    high = weight.astype(jnp.bfloat16)
    low = (weight - high.astype(jnp.float32)).astype(jnp.bfloat16)
    return layer(
        q, kv, out_weight, gate_weight, up_weight, down_weight,
        jnp.concatenate([high, low], axis=1), lambdas.reshape(1, 1),
        head_gain.reshape(1, LANES), select, residual, norm_gain.reshape(1, DEPTH),
    )


def solution(mesh):
    in_specs = (
        P("sp", "tp", None),
        P("sp", "tp", None),
        P("sp", "tp", None),
        P("tp"),
        P(),
        P(),
        P(("sp", "tp"), None),
        P(),
        P(("sp", "tp"), None),
        P(("sp", "tp"), None),
        P("sp", None, "tp"),
        P("sp", None, "tp"),
        P("sp", "tp", None),
    )
    return jax.shard_map(
        shards, mesh=mesh, in_specs=in_specs, out_specs=P(("sp", "tp"), None), check_vma=False
    )
```

```python
import jax
import jax.numpy as jnp
from jax import lax
from jax.experimental import pallas as pl
from jax.experimental.pallas import tpu as pltpu
from jax.sharding import PartitionSpec as P

MESH = pl.DeviceIdType.MESH
SIDE = 4
N_SP = 16
N_TP = 16
ROWS = 48
SPAN = N_TP * ROWS
HALF = SPAN // 2
LANES = 128
TILES = SPAN // LANES
ONES = 16
HD = 64
DEPTH = 2048
EXPERTS = 32
CAP = 4
SLOTS = EXPERTS * CAP
COLS = 512
NEG = -1e30

ORDER = [
    (0, 0), (-1, 0), (1, 0), (0, -1), (0, 1), (2, 0), (-1, -1), (-1, 1),
    (1, -1), (1, 1), (2, -1), (2, 1), (0, 2), (-1, 2), (1, 2), (2, 2),
]
PLACE = {0: 0, -1: 1, 1: 2, 2: 3}


def pick(index, values):
    out = jnp.int32(values[0])
    for k, value in enumerate(values):
        out = jnp.where(index == k, jnp.int32(value), out)
    return out


def mod(value, size):
    return lax.rem(value + size, size)


def attend_part(
    lam_ref, gain_ref, select_ref, residual_ref, norm_gain_ref,
    load_q, load_kv, load_w, send_comb, owner, keeps,
    updated_ref, slots_ref,
    q_own, q_land, qs, kvb, acc, top, score_a, score_b, weight_a, weight_b,
    own_heads, heads, w_vmem,
    q_send, q_recv, kv_send, kv_recv, head_send, head_recv,
):
    sp = lax.axis_index("sp")
    tp = lax.axis_index("tp")
    x, y = lax.rem(sp, SIDE), sp // SIDE

    load_q.wait()

    def row_block(g):
        return pl.ds(pl.multiple_of(g * ROWS, ROWS), ROWS)

    def q_copy(d):
        other = lax.rem(sp + d, N_SP)
        return pltpu.make_async_remote_copy(
            src_ref=q_own.at[owner(other, sp)], dst_ref=q_land.at[row_block(sp)],
            send_sem=q_send.at[d], recv_sem=q_recv.at[d],
            device_id=(other, tp), device_id_type=MESH,
        )

    def send_q(d, carry):
        q_copy(d).start()
        return carry

    lax.fori_loop(1, N_SP, send_q, 0)
    load_kv.wait()

    def block_of(half, du, dv):
        dx, dy = (du, dv) if half == 0 else (dv, du)
        return mod(y + dy, SIDE) * SIDE + mod(x + dx, SIDE)

    def kv_copy(half, index, block, part, du, dv):
        ref = kvb.at[block, half] if part is None else kvb.at[block, half, part]
        return pltpu.make_async_remote_copy(
            src_ref=ref, dst_ref=ref,
            send_sem=kv_send.at[half, index], recv_sem=kv_recv.at[half, index],
            device_id=(block_of(half, du, dv), tp), device_id_type=MESH,
        )

    def send(half, index, rel, part, du, dv):
        kv_copy(half, index, block_of(half, *rel), part, du, dv).start()

    def arrived(half, index, rel, part):
        kv_copy(half, index, block_of(half, *rel), part, 1, 0).wait_recv()

    for half in range(2):
        send(half, 0, (0, 0), None, 1, 0)
        send(half, 1, (0, 0), None, -1, 0)
        send(half, 4, (0, 0), None, 0, 1)
        send(half, 8, (0, 0), None, 0, -1)
    send_comb()

    for own in range(N_SP):
        @pl.when(sp == own)
        def _():
            q_land[own * ROWS : (own + 1) * ROWS] = q_own[2 * own % N_TP]

    def wait_q(d, carry):
        q_copy(d).wait_recv()
        return carry

    lax.fori_loop(1, N_SP, wait_q, 0)

    lane = lax.broadcasted_iota(jnp.int32, (LANES, LANES), 1)
    for i in range(TILES):
        wide = q_land[i * LANES : (i + 1) * LANES].astype(jnp.float32) * (HD**-0.5)
        qs[i, 0:LANES] = jnp.where(lane < HD, wide, 0.0).astype(jnp.bfloat16)
        qs[i, LANES : 2 * LANES] = jnp.where(lane >= HD, wide, 0.0).astype(jnp.bfloat16)
    acc[...] = jnp.zeros_like(acc)
    top[...] = jnp.full_like(top, NEG)

    score_bufs, weight_bufs = (score_a, score_b), (weight_a, weight_b)

    def tiles_step(first, block, half):
        keys = kvb[block, half, 0]
        wide = jnp.concatenate(
            [kvb[block, half, 1, k * LANES : (k + 1) * LANES] for k in range(HALF // LANES)],
            axis=1,
        )
        wide = jnp.concatenate([wide, jnp.ones((ONES, HALF), jnp.bfloat16)], axis=0)

        def score(i):
            scores = lax.dot_general(
                keys, qs[i], (((1,), (1,)), ((), ())), preferred_element_type=jnp.float32
            )
            if i < first + 3:
                place = lax.broadcasted_iota(jnp.int32, (1, LANES), 1) + i * LANES
                span = lax.shift_right_logical(place * 1366, 16)
                last = (
                    span * (SPAN - ROWS) + place + ((sp + span) & (N_TP - 1)) * ROWS
                    - block * SPAN - half * HALF
                )
                kept = lax.broadcasted_iota(jnp.int32, (HALF, LANES), 0) <= last
                scores = jnp.where(jnp.concatenate([kept, kept], axis=1), scores, -jnp.inf)
            score_bufs[i % 2][...] = scores
            old_top = top[i]
            new_top = jnp.maximum(old_top, jnp.max(scores, axis=0, keepdims=True))
            top[i] = new_top
            return new_top, jnp.exp(old_top - new_top)

        def weigh(i, new_top):
            weights = jnp.exp(score_bufs[i % 2][...] - new_top)
            weight_bufs[i % 2][...] = weights.astype(jnp.bfloat16)

        def add_up(i, decay):
            fresh = jnp.dot(wide, weight_bufs[i % 2][...], preferred_element_type=jnp.float32)
            acc[i] = acc[i] * decay + fresh

        state = {first: score(first)}
        for i in range(first, TILES + 1):
            if i + 1 < TILES:
                state[i + 1] = score(i + 1)
            if i < TILES:
                weigh(i, state[i][0])
            if i > first:
                add_up(i - 1, state[i - 1][1])

    def use_block(block, half):
        first = block * ROWS // LANES // 2
        for k in range(TILES // 2):
            @pl.when(first == k)
            def _():
                tiles_step(2 * k, block, half)

    def step(s, carry):
        def on(k, half):
            du, dv = ORDER[k]
            if k == 1:
                arrived(half, 0, (-1, 0), None)
                send(half, 2, (-1, 0), 0, 1, 0)
                send(half, 5, (-1, 0), None, 0, 1)
                send(half, 9, (-1, 0), None, 0, -1)
            elif k == 2:
                arrived(half, 1, (1, 0), None)
                send(half, 3, (1, 0), 1, -1, 0)
                send(half, 6, (1, 0), None, 0, 1)
                send(half, 10, (1, 0), None, 0, -1)
            elif k == 5:
                arrived(half, 2, (2, 0), 0)
                arrived(half, 3, (2, 0), 1)
                send(half, 7, (2, 0), None, 0, 1)
                send(half, 11, (2, 0), None, 0, -1)
            elif dv == -1:
                place = PLACE[du]
                arrived(half, 4 + place, (du, dv), None)
                send(half, 12 + place, (du, dv), 0, 0, 1)
            elif dv == 1:
                place = PLACE[du]
                arrived(half, 8 + place, (du, dv), None)
                send(half, 16 + place, (du, dv), 1, 0, -1)
            elif dv == 2:
                place = PLACE[du]
                arrived(half, 12 + place, (du, dv), 0)
                arrived(half, 16 + place, (du, dv), 1)

        for k in range(1, len(ORDER)):
            @pl.when(s == k)
            def _():
                for half in range(2):
                    on(k, half)

        du = pick(s, [o[0] for o in ORDER])
        dv = pick(s, [o[1] for o in ORDER])

        def one_half(half, carry):
            dx = jnp.where(half == 0, du, dv)
            dy = jnp.where(half == 0, dv, du)
            block = mod(y + dy, SIDE) * SIDE + mod(x + dx, SIDE)
            use_block(block, half)
            return carry

        return lax.fori_loop(0, 2, one_half, carry)

    lax.fori_loop(0, len(ORDER), step, 0)

    lam = lam_ref[0, 0]

    for i in range(TILES):
        ratio = acc[i, 0:LANES] / acc[i, LANES : LANES + 1]
        mixed = ratio[:, 0:LANES] - lam * ratio[:, LANES : 2 * LANES]
        square = jnp.mean(mixed * mixed, axis=0, keepdims=True)
        done = (mixed * lax.rsqrt(square + 1e-06)).T * gain_ref[...]
        own_heads[i * LANES : (i + 1) * LANES] = done.astype(jnp.bfloat16)

    def head_copy(g, h):
        return pltpu.make_async_remote_copy(
            src_ref=own_heads.at[row_block(g)],
            dst_ref=heads.at[:, pl.ds(pl.multiple_of(tp * LANES, LANES), LANES)],
            send_sem=head_send.at[g], recv_sem=head_recv.at[h],
            device_id=(g, owner(sp, g)), device_id_type=MESH,
        )

    def push_head(g, carry):
        @pl.when(jnp.logical_or(g != sp, jnp.logical_not(keeps)))
        def _():
            head_copy(g, tp).start()

        return carry

    lax.fori_loop(0, N_SP, push_head, 0)

    for own in range(N_SP):
        @pl.when(jnp.logical_and(sp == own, keeps))
        def _():
            at = 2 * own % N_TP * LANES
            heads[:, at : at + LANES] = own_heads[own * ROWS : (own + 1) * ROWS]

    load_w.wait()

    def wait_head(h, carry):
        @pl.when(jnp.logical_or(h != tp, jnp.logical_not(keeps)))
        def _():
            head_copy(0, h).wait_recv()

        return carry

    lax.fori_loop(0, N_TP, wait_head, 0)

    attended = heads[...]
    squares = jnp.zeros((ROWS, 1), jnp.float32)
    wide = []
    for n in range(DEPTH // COLS):
        cols = slice(n * COLS, (n + 1) * COLS)
        projected = jnp.dot(attended, w_vmem[:, cols], preferred_element_type=jnp.float32)
        updated = (residual_ref[:, cols].astype(jnp.float32) + projected).astype(jnp.bfloat16)
        updated_ref[:, cols] = updated
        back = updated.astype(jnp.float32)
        squares = squares + jnp.sum(back * back, axis=1, keepdims=True)
        wide.append(back)
    scale = lax.rsqrt(squares / DEPTH + 1e-06)
    for n in range(DEPTH // COLS):
        cols = slice(n * COLS, (n + 1) * COLS)
        normed = (wide[n] * scale * norm_gain_ref[:, cols]).astype(jnp.bfloat16)
        packed = lax.dot_general(
            select_ref[...], normed, (((0,), (0,)), ((), ())), preferred_element_type=jnp.float32
        )
        slots_ref[:, :, cols] = packed.reshape(N_SP, 8, COLS).astype(jnp.bfloat16)

    def drain():
        def drain_q(d, carry):
            q_copy(d).wait_send()
            return carry

        lax.fori_loop(1, N_SP, drain_q, 0)

        def drain_heads(g, carry):
            @pl.when(jnp.logical_or(g != sp, jnp.logical_not(keeps)))
            def _():
                head_copy(g, tp).wait_send()

            return carry

        lax.fori_loop(0, N_SP, drain_heads, 0)
        for half in range(2):
            for index in range(20):
                part = None if index in (0, 1) or 4 <= index < 12 else 0
                kv_copy(half, index, sp, part, 1, 0).wait_send()

    return drain


RING = 8
PIECE = 8
WIDE = 2 * LANES
EARLY = 1536
LATE = DEPTH - EARLY
PARTS = 4
PART = EARLY // PARTS
LATE_PART = LATE // 2
Z_ORDER = [0, -1, 1, -2, 2, -3, 3, 4]
SPREAD = [0, 1, 3, 4, 12, 5, 7, 8, 13, 15, 2, 6, 9, 11, 14, 10]
Z_PLACE = {d: k for k, d in enumerate(Z_ORDER)}


def expert_part(
    slots_own, updated_ref, loads, comb_copy,
    merged_ref,
    rows, gate_up, down, comb, own_part, pair_out, pair_in, out,
    res, red, sum_out, sum_in, tail_out, tail_in, whole_out, whole_in,
    slot_send, slot_recv, ring_send, ring_recv, fwd_send, fwd_recv,
    pair_send, pair_recv, res_send, res_recv, sum_send, sum_recv,
    tail_send, tail_recv, whole_send, whole_recv,
):
    sp = lax.axis_index("sp")
    tp = lax.axis_index("tp")
    z, core = tp // 2, lax.rem(tp, 2)
    x, y = lax.rem(sp, SIDE), sp // SIDE

    def at_z(dz):
        return (sp, 2 * mod(z + dz, RING) + core)

    partner = (sp, 2 * z + (1 - core))

    def remote(src, dst, send_sem, recv_sem, device):
        return pltpu.make_async_remote_copy(
            src_ref=src, dst_ref=dst, send_sem=send_sem, recv_sem=recv_sem,
            device_id=device, device_id_type=MESH,
        )

    def peer(d):
        return mod(y + d // SIDE, SIDE) * SIDE + mod(x + lax.rem(d, SIDE), SIDE)

    def slot_copy(d):
        other = peer(d)
        return remote(
            slots_own.at[other], rows.at[tp, sp], slot_send.at[d], slot_recv.at[d], (other, tp)
        )

    def send_slot(n, carry):
        slot_copy(pick(n, SPREAD)).start()
        return carry

    lax.fori_loop(1, N_SP, send_slot, 0)
    rows[tp, sp] = slots_own[sp]
    for item in loads:
        item.wait()

    def ring_copy(way, m, dz, piece):
        ref = rows.at[2 * mod(z + dz, RING) + core, pl.ds(piece * PIECE, PIECE)]
        return remote(
            ref, ref, ring_send.at[way, m], ring_recv.at[way, m], at_z(1 if way == 0 else -1)
        )

    def fwd_copy(j, dz):
        ref = rows.at[2 * mod(z + dz, RING) + core]
        return remote(ref, ref, fwd_send.at[j], fwd_recv.at[j], partner)

    def pair_copy(j):
        return remote(pair_out.at[j], pair_in.at[j], pair_send.at[j], pair_recv.at[j], partner)

    def res_copy(j, d):
        other = peer(d)
        return remote(
            out.at[j, other, :, 0:EARLY], res.at[j, sp, :, 0:EARLY],
            res_send.at[j, d], res_recv.at[j, d], (other, tp),
        )

    def ring_event(k):
        if k == 0:
            for piece in range(2):
                def wait_slot(src, carry):
                    d = mod(y - src // SIDE, SIDE) * SIDE + mod(x - lax.rem(src, SIDE), SIDE)

                    @pl.when(d != 0)
                    def _():
                        slot_copy(d).wait_recv()

                    return carry

                lax.fori_loop(piece * PIECE, (piece + 1) * PIECE, wait_slot, 0)
                for way in range(2):
                    ring_copy(way, piece, 0, piece).start()
            fwd_copy(0, 0).start()
        elif k < 4:
            for piece in range(2):
                for way in range(2):
                    dz = -k if way == 0 else k
                    ring_copy(way, 2 * (k - 1) + piece, dz, piece).wait_recv()
                    if k < 3:
                        ring_copy(way, 2 * k + piece, dz, piece).start()
                    elif piece == way:
                        ring_copy(way, 6, dz, piece).start()
            fwd_copy(2 * k - 1, -k).start()
            fwd_copy(2 * k, k).start()
        else:
            ring_copy(0, 6, 4, 0).wait_recv()
            ring_copy(1, 6, 4, 1).wait_recv()
            fwd_copy(7, 4).start()

    row_expert = lax.rem(lax.broadcasted_iota(jnp.int32, (2 * N_SP * CAP, WIDE), 0), 8) // CAP
    col_expert = lax.broadcasted_iota(jnp.int32, (2 * N_SP * CAP, WIDE), 1) // LANES
    mine = row_expert == col_expert

    def chunk_part(chunk, dst, j):
        x = rows[chunk].reshape(2 * N_SP * CAP, DEPTH)
        gate = jnp.dot(x, gate_up[:, 0:WIDE], preferred_element_type=jnp.float32)
        up = jnp.dot(x, gate_up[:, WIDE : 2 * WIDE], preferred_element_type=jnp.float32)
        inner = gate / (1.0 + jnp.exp(-gate)) * up
        inner = jnp.where(mine, inner, 0.0).astype(jnp.bfloat16)
        for n in range(DEPTH // COLS):
            cols = slice(n * COLS, (n + 1) * COLS)
            piece = jnp.dot(inner, down[:, cols], preferred_element_type=jnp.float32)
            dst[j, :, :, cols] = piece.reshape(N_SP, 8, COLS).astype(jnp.bfloat16)

    def push_results(j):
        pair_copy(j).wait_recv()
        total = own_part[j].astype(jnp.float32) + pair_in[j].astype(jnp.float32)
        out[j] = total.astype(jnp.bfloat16)
        res[j, sp, :, 0:EARLY] = out[j, sp, :, 0:EARLY]

        def push(n, carry):
            res_copy(j, pick(n, SPREAD)).start()
            return carry

        lax.fori_loop(1, N_SP, push, 0)

    def combine(j):
        def wait_res(d, carry):
            res_copy(j, d).wait_recv()
            return carry

        lax.fori_loop(1, N_SP, wait_res, 0)
        zj = mod(z + pick(j, Z_ORDER), RING)

        @pl.when(zj != z)
        def _():
            comb_copy(mod(z - zj, RING)).wait_recv()

        high, low = comb[zj, :, 0:LANES], comb[zj, :, LANES:WIDE]
        for n in range(EARLY // COLS):
            cols = slice(n * COLS, (n + 1) * COLS)
            found = res[j, :, :, cols].reshape(SLOTS, COLS)
            red[j, :, cols] = jnp.dot(
                high, found, preferred_element_type=jnp.float32
            ) + jnp.dot(low, found, preferred_element_type=jnp.float32)

    def tail_copy(way, r, h):
        cols = slice(h * LATE_PART, (h + 1) * LATE_PART)
        return remote(
            tail_out.at[way, r, :, :, cols], tail_in.at[way, r, :, :, cols],
            tail_send.at[way, r, h], tail_recv.at[way, r, h], at_z(-1 if way == 0 else 1),
        )

    def tail_step(way, r, h):
        cols = slice(h * LATE_PART, (h + 1) * LATE_PART)
        d = 4 if r == 0 else (r - 4 if way == 0 else 4 - r)
        value = out[Z_PLACE[d], :, :, EARLY + h * LATE_PART : EARLY + (h + 1) * LATE_PART]
        if r > 1 or (r == 1 and h == way):
            tail_copy(way, r - 1, h).wait_recv()
            there = tail_in[way, r - 1, :, :, cols].astype(jnp.float32)
            value = (value.astype(jnp.float32) + there).astype(jnp.bfloat16)
        tail_out[way, r, :, :, cols] = value
        tail_copy(way, r, h).start()

    def tail_steps(r, some):
        for way in range(2):
            tail_step(way, r, way if some else 1 - way)

    def whole_copy(d):
        other = peer(d)
        return remote(
            whole_out.at[other], whole_in.at[sp], whole_send.at[d], whole_recv.at[d], (other, tp)
        )

    def push_whole():
        for h in range(2):
            cols = slice(h * LATE_PART, (h + 1) * LATE_PART)
            at = slice(EARLY + h * LATE_PART, EARLY + (h + 1) * LATE_PART)
            total = out[0, :, :, at].astype(jnp.float32)
            for way in range(2):
                tail_copy(way, 3, h).wait_recv()
                total = total + tail_in[way, 3, :, :, cols].astype(jnp.float32)
            whole_out[:, :, cols] = total.astype(jnp.bfloat16)
        whole_in[sp] = whole_out[sp]

        def push(n, carry):
            whole_copy(pick(n, SPREAD)).start()
            return carry

        lax.fori_loop(1, N_SP, push, 0)

    def sum_copy(way, r, h):
        cols = slice(h * PART, (h + 1) * PART)
        return remote(
            sum_out.at[way, r, :, cols], sum_in.at[way, r, :, cols],
            sum_send.at[way, r, h], sum_recv.at[way, r, h], at_z(-1 if way == 0 else 1),
        )

    def far(way, h):
        return (h >= PARTS // 2) == (way == 1)

    def sum_steps(r, some):
        for h in range(PARTS // 2):
            for way in range(2):
                sum_step(way, r, h + PARTS // 2 * int((way == 1) == some))

    def sum_step(way, r, h):
        cols = slice(h * PART, (h + 1) * PART)
        d = 4 if r == 0 else (r - 4 if way == 0 else 4 - r)
        value = red[Z_PLACE[d], :, cols]
        if r > 1 or (r == 1 and far(way, h)):
            sum_copy(way, r - 1, h).wait_recv()
            value = value + sum_in[way, r - 1, :, cols].astype(jnp.float32)
        sum_out[way, r, :, cols] = value.astype(jnp.bfloat16)
        sum_copy(way, r, h).start()

    def pair_round(first, last):
        def one(j, carry):
            zj = mod(z + pick(j, Z_ORDER), RING)
            chunk_part(2 * zj + core, own_part, j)
            fwd_copy(j, 0).wait_recv()
            chunk_part(2 * zj + (1 - core), pair_out, j)
            pair_copy(j).start()

            @pl.when(j > first)
            def _():
                push_results(first)

            return carry

        lax.fori_loop(first, last + 1, one, 0)
        push_results(last)

    def combine_some(first, last):
        def one(j, carry):
            combine(j)
            return carry

        lax.fori_loop(first, last + 1, one, 0)

    def step(k, carry):
        for at in range(5):
            @pl.when(k == at)
            def _():
                ring_event(at)

        last = jnp.minimum(2 * k, RING - 1)
        pair_round(jnp.maximum(2 * k - 1, 0), last)

        @pl.when(jnp.logical_or(k == 2, k == 3))
        def _():
            combine_some(jnp.maximum(2 * k - 5, 0), 2 * k - 4)

        return carry

    lax.fori_loop(0, 5, step, 0)
    tail_steps(1, False)
    tail_steps(0, True)
    combine_some(3, 4)
    tail_steps(2, False)
    tail_steps(1, True)
    combine_some(5, 5)
    tail_steps(3, False)
    tail_steps(2, True)
    combine_some(6, 6)
    tail_steps(3, True)
    sum_steps(1, False)
    combine_some(7, 7)
    sum_steps(0, True)
    push_whole()
    sum_steps(2, False)
    sum_steps(1, True)
    sum_steps(3, False)
    sum_steps(2, True)
    sum_steps(3, True)

    def wait_whole(d, carry):
        whole_copy(d).wait_recv()
        return carry

    lax.fori_loop(1, N_SP, wait_whole, 0)
    found = whole_in[...].reshape(SLOTS, LATE)
    total = updated_ref[:, EARLY:DEPTH].astype(jnp.float32)
    for part in (comb[z, :, 0:LANES], comb[z, :, LANES:WIDE]):
        total = total + jnp.dot(part, found, preferred_element_type=jnp.float32)
    merged_ref[:, EARLY:DEPTH] = total.astype(jnp.bfloat16)
    for h in range(PARTS):
        cols = slice(h * PART, (h + 1) * PART)
        total = updated_ref[:, cols].astype(jnp.float32) + red[0, :, cols]
        for way in range(2):
            sum_copy(way, 3, h).wait_recv()
            total = total + sum_in[way, 3, :, cols].astype(jnp.float32)
        merged_ref[:, cols] = total.astype(jnp.bfloat16)

    def drain_plane(d, carry):
        slot_copy(d).wait_send()
        whole_copy(d).wait_send()

        def drain_res(j, inner):
            res_copy(j, d).wait_send()
            return inner

        return lax.fori_loop(0, RING, drain_res, carry)

    lax.fori_loop(1, N_SP, drain_plane, 0)

    def drain_pair(j, carry):
        fwd_copy(j, 0).wait_send()
        pair_copy(j).wait_send()
        return carry

    lax.fori_loop(0, RING, drain_pair, 0)
    for way in range(2):
        for m in range(7):
            ring_copy(way, m, 0, 0).wait_send()
        for r in range(4):
            for h in range(2):
                if r > 0 or h == way:
                    tail_copy(way, r, h).wait_send()
            for h in range(PARTS):
                if r > 0 or far(way, h):
                    sum_copy(way, r, h).wait_send()


def layer_kernel(
    q_hbm, kv_hbm, w_hbm, gate_hbm, up_hbm, down_hbm, comb_hbm,
    lam_ref, gain_ref, select_ref, residual_ref, norm_gain_ref,
    merged_ref,
    *scratch,
):
    (q_own, q_land, qs, kvb, acc, top, score_a, score_b, weight_a, weight_b,
     own_heads, heads, w_vmem, updated_ref, slots_own,
     rows, gate_up, down, comb_own, comb, own_part, pair_out, pair_in, out,
     res, red, sum_out, sum_in, tail_out, tail_in, whole_out, whole_in,
     local_sem, q_send, q_recv, kv_send, kv_recv, head_send, head_recv,
     slot_send, slot_recv, ring_send, ring_recv, fwd_send, fwd_recv,
     pair_send, pair_recv, res_send, res_recv, comb_send, comb_recv, sum_send, sum_recv,
     tail_send, tail_recv, whole_send, whole_recv) = scratch
    sp = lax.axis_index("sp")
    tp = lax.axis_index("tp")
    z, core = tp // 2, lax.rem(tp, 2)

    barrier = pltpu.get_barrier_semaphore()

    def load(k, src, dst):
        return pltpu.make_async_copy(src, dst, local_sem.at[k])

    load_q = load(0, q_hbm, q_own)
    load_kv = load(1, kv_hbm, kvb.at[sp])
    load_comb = [load(2, comb_hbm, comb_own), load(3, comb_hbm, comb.at[z])]
    load_w = load(4, w_hbm, w_vmem)
    loads = []
    for e in range(2):
        loads += [
            load(5 + e, gate_hbm.at[e], gate_up.at[:, e * LANES : (e + 1) * LANES]),
            load(7 + e, up_hbm.at[e], gate_up.at[:, (2 + e) * LANES : (3 + e) * LANES]),
            load(9 + e, down_hbm.at[e], down.at[e * LANES : (e + 1) * LANES]),
        ]
    for item in [load_q, load_kv, *load_comb, load_w, *loads]:
        item.start()

    def greet(*device):
        pl.semaphore_signal(barrier, inc=1, device_id=device, device_id_type=MESH)

    def greet_plane(d, carry):
        greet(lax.rem(sp + d, N_SP), tp)
        return carry

    lax.fori_loop(1, N_SP, greet_plane, 0)

    def owner(i, b):
        return lax.rem(i + b, N_TP)

    source = mod(tp - sp, N_SP)
    keeps = owner(sp, sp) == tp

    def greet_sources(h, carry):
        @pl.when(jnp.logical_or(jnp.logical_not(keeps), h != tp))
        def _():
            greet(source, h)

        return carry

    lax.fori_loop(0, N_TP, greet_sources, 0)

    def plane_z(d):
        return 2 * lax.rem(z + d, RING) + core

    def greet_ring(d, carry):
        greet(sp, plane_z(d))
        return carry

    lax.fori_loop(1, RING, greet_ring, 0)
    greet(sp, 2 * z + (1 - core))
    pl.semaphore_wait(
        barrier,
        N_SP - 1 + N_TP + RING - jnp.where(keeps, jnp.int32(1), jnp.int32(0)),
    )

    def comb_copy(d):
        return pltpu.make_async_remote_copy(
            src_ref=comb_own, dst_ref=comb.at[z],
            send_sem=comb_send.at[d], recv_sem=comb_recv.at[d],
            device_id=(sp, plane_z(d)), device_id_type=MESH,
        )

    def send_comb():
        for item in load_comb:
            item.wait()

        def one(d, carry):
            comb_copy(d).start()
            return carry

        lax.fori_loop(1, RING, one, 0)

    drain_attend = attend_part(
        lam_ref, gain_ref, select_ref, residual_ref, norm_gain_ref,
        load_q, load_kv, load_w, send_comb, owner, keeps,
        updated_ref, slots_own,
        q_own, q_land, qs, kvb, acc, top, score_a, score_b, weight_a, weight_b,
        own_heads, heads, w_vmem,
        q_send, q_recv, kv_send, kv_recv, head_send, head_recv,
    )
    expert_part(
        slots_own, updated_ref, loads, comb_copy,
        merged_ref,
        rows, gate_up, down, comb, own_part, pair_out, pair_in, out,
        res, red, sum_out, sum_in, tail_out, tail_in, whole_out, whole_in,
        slot_send, slot_recv, ring_send, ring_recv, fwd_send, fwd_recv,
        pair_send, pair_recv, res_send, res_recv, sum_send, sum_recv,
        tail_send, tail_recv, whole_send, whole_recv,
    )
    drain_attend()

    def drain_comb(d, carry):
        comb_copy(d).wait_send()
        return carry

    lax.fori_loop(1, RING, drain_comb, 0)


def layer(q, kv, w, gate, up, down, comb, lam, gain, select, residual, norm_gain):
    anywhere = pl.BlockSpec(memory_space=pl.ANY)
    vmem = pl.BlockSpec(memory_space=pltpu.VMEM)
    smem = pl.BlockSpec(memory_space=pltpu.SMEM)
    dma = pltpu.SemaphoreType.DMA
    chunk = (N_SP, 8, DEPTH)
    bf16, f32 = jnp.bfloat16, jnp.float32
    return pl.pallas_call(
        layer_kernel,
        out_shape=jax.ShapeDtypeStruct((ROWS, DEPTH), bf16),
        in_specs=[anywhere] * 7 + [smem, vmem, vmem, vmem, vmem],
        out_specs=vmem,
        scratch_shapes=[
            pltpu.VMEM((N_SP, ROWS, LANES), bf16),
            pltpu.VMEM((SPAN, LANES), bf16),
            pltpu.VMEM((TILES, 2 * LANES, LANES), bf16),
            pltpu.VMEM((N_SP, 2, 2, HALF, LANES), bf16),
            pltpu.VMEM((TILES, LANES + ONES, 2 * LANES), f32),
            pltpu.VMEM((TILES, 1, 2 * LANES), f32),
            pltpu.VMEM((HALF, 2 * LANES), f32),
            pltpu.VMEM((HALF, 2 * LANES), f32),
            pltpu.VMEM((HALF, 2 * LANES), bf16),
            pltpu.VMEM((HALF, 2 * LANES), bf16),
            pltpu.VMEM((SPAN, LANES), bf16),
            pltpu.VMEM((ROWS, DEPTH), bf16),
            pltpu.VMEM((DEPTH, DEPTH), bf16),
            pltpu.VMEM((ROWS, DEPTH), bf16),
            pltpu.VMEM(chunk, bf16),
            pltpu.VMEM((N_TP, *chunk), bf16),
            pltpu.VMEM((DEPTH, 2 * WIDE), bf16),
            pltpu.VMEM((WIDE, DEPTH), bf16),
            pltpu.VMEM((ROWS, WIDE), bf16),
            pltpu.VMEM((RING, ROWS, WIDE), bf16),
            pltpu.VMEM((RING, *chunk), bf16),
            pltpu.VMEM((RING, *chunk), bf16),
            pltpu.VMEM((RING, *chunk), bf16),
            pltpu.VMEM((RING, *chunk), bf16),
            pltpu.VMEM((RING, *chunk), bf16),
            pltpu.VMEM((RING, ROWS, EARLY), f32),
            pltpu.VMEM((2, 4, ROWS, EARLY), bf16),
            pltpu.VMEM((2, 4, ROWS, EARLY), bf16),
            pltpu.VMEM((2, 4, N_SP, 8, LATE), bf16),
            pltpu.VMEM((2, 4, N_SP, 8, LATE), bf16),
            pltpu.VMEM((N_SP, 8, LATE), bf16),
            pltpu.VMEM((N_SP, 8, LATE), bf16),
            dma((11,)),
            dma((N_SP,)),
            dma((N_SP,)),
            dma((2, 20)),
            dma((2, 20)),
            dma((N_SP,)),
            dma((N_TP,)),
            dma((N_SP,)),
            dma((N_SP,)),
            dma((2, 7)),
            dma((2, 7)),
            dma((RING,)),
            dma((RING,)),
            dma((RING,)),
            dma((RING,)),
            dma((RING, N_SP)),
            dma((RING, N_SP)),
            dma((RING,)),
            dma((RING,)),
            dma((2, 4, PARTS)),
            dma((2, 4, PARTS)),
            dma((2, 4, 2)),
            dma((2, 4, 2)),
            dma((N_SP,)),
            dma((N_SP,)),
        ],
        compiler_params=pltpu.CompilerParams(
            collective_id=0, has_side_effects=True, vmem_limit_bytes=63 * 1024 * 1024
        ),
        name="layer",
    )(q, kv, w, gate, up, down, comb, lam, gain, select, residual, norm_gain)


def shards(
    queries, key_pairs, head_values, lambdas, head_gain, out_weight, residual, norm_gain,
    expert_ids, route_weights, gate_weight, up_weight, down_weight,
):
    q = queries.reshape(N_SP, ROWS, LANES)
    across = head_values.reshape(SPAN // LANES, LANES, LANES).swapaxes(1, 2)
    kv = jnp.stack(
        [key_pairs.reshape(2, HALF, LANES), across.reshape(2, HALF, LANES)], axis=1
    )
    slot = jnp.arange(SLOTS, dtype=jnp.int32)[None, :]
    first, second = (expert_ids[:, c : c + 1] == slot // CAP for c in range(2))
    named = first | second
    earlier = jnp.tri(ROWS, k=-1, dtype=jnp.bfloat16)
    rank = jnp.dot(earlier, named.astype(jnp.bfloat16), preferred_element_type=jnp.float32)
    hit = named & (rank == (slot % CAP).astype(jnp.float32))
    select = hit.astype(jnp.bfloat16)
    weight = jnp.where(first, route_weights[:, 0:1], route_weights[:, 1:2])
    weight = jnp.where(hit, weight, 0.0)
    high = weight.astype(jnp.bfloat16)
    low = (weight - high.astype(jnp.float32)).astype(jnp.bfloat16)
    return layer(
        q, kv, out_weight, gate_weight, up_weight, down_weight,
        jnp.concatenate([high, low], axis=1), lambdas.reshape(1, 1),
        head_gain.reshape(1, LANES), select, residual, norm_gain.reshape(1, DEPTH),
    )


def solution(mesh):
    in_specs = (
        P("sp", "tp", None),
        P("sp", "tp", None),
        P("sp", "tp", None),
        P("tp"),
        P(),
        P(),
        P(("sp", "tp"), None),
        P(),
        P(("sp", "tp"), None),
        P(("sp", "tp"), None),
        P("sp", None, "tp"),
        P("sp", None, "tp"),
        P("sp", "tp", None),
    )
    return jax.shard_map(
        shards, mesh=mesh, in_specs=in_specs, out_specs=P(("sp", "tp"), None), check_vma=False
    )
```
